32 devices in a mesh: sp: 8 (over z, y), tp: 4 (over x, core).
Axes of the slice: x: 2, y: 2, z: 4, core: 2. Of those that a mesh axis runs over, the one named last changes fastest.
Arguments:
- tokens: bfloat16 [1280, 2048], P('sp'), may hold values from -6 to 6
- input_gain: float32 [2048], replicated, may hold values from 0.1 to 1.9
- chain_query: bfloat16 [2048, 1024], P('sp', 'tp'), may hold values from -0.125 to 0.125
- forward_gate: bfloat16 [2048, 1024], P('sp', 'tp'), may hold values from -0.125 to 0.125
- backward_gate: bfloat16 [2048, 1024], P('sp', 'tp'), may hold values from -0.125 to 0.125
- chain_value: bfloat16 [2048, 1024], P('sp', 'tp'), may hold values from -0.125 to 0.125
- output_gate: bfloat16 [2048, 1024], P('sp', 'tp'), may hold values from -0.125 to 0.125
- forget_rate: float32 [2, 1024], P(None, 'tp'), may hold values from 0.2 to 6
- chain_gain: float32 [1024], P('tp'), may hold values from 0.1 to 1.9
- query_down: bfloat16 [2048, 768], P('sp'), may hold values from -0.125 to 0.125
- latent_down: bfloat16 [2048, 512], P('sp'), may hold values from -0.125 to 0.125
- rotary_down: bfloat16 [2048, 64], replicated, may hold values from -0.125 to 0.125
- query_latent_gain: float32 [768], replicated, may hold values from 0.1 to 1.9
- latent_gain: float32 [512], replicated, may hold values from 0.1 to 1.9
- query_up: bfloat16 [768, 1536], P(None, 'tp'), may hold values from -0.21875 to 0.21875
- latent_up: bfloat16 [512, 2048], P(None, 'tp'), may hold values from -0.25 to 0.25
- query_head_gain: float32 [192], replicated, may hold values from 0.1 to 1.9
- key_head_gain: float32 [192], replicated, may hold values from 0.1 to 1.9
- mixer_gain: float32 [1024], P('tp'), may hold values from 0.1 to 1.9
- chain_out: bfloat16 [1024, 2048], P('tp', 'sp'), may hold values from -0.125 to 0.125
- attend_out: bfloat16 [1024, 2048], P('tp', 'sp'), may hold values from -0.125 to 0.125
Outputs:
- mixed: float32 [1280, 2048], P(('sp', 'tp'))
The draws below stay inside these ranges and needn't reach their ends.
All inputs are finite; a program needn't handle non-finite values.
Results may differ from the reference program's by a relative error of at most 0.017.
Values may be sent and summed in bfloat16 or wider, within the bound.
A program may use at most 128 MiB of HBM per device.

```python
import math
import jax
import jax.numpy as jnp
from jax import lax

D = 2048
KEY_DIM = 128
VAL_DIM = 128
HEADS_ATT = 8
NOPE_DIM = 128
ROPE_DIM = 64
VHEAD_DIM = 128
QLAT = 768
KVLAT = 512
TOK_DEV = 160
SEQ = 1280
REC_KEYS = 1024
REC_WIDTH = 1024
ATT_QK = 192
ATT_WIDTH = 1024


def block_levels(key, shape, cuts, low, top_value):
    factor_of = 1.0
    for dim, parts in cuts:
        draws = jax.random.uniform(jax.random.fold_in(jax.random.fold_in(key, 6), dim), (parts,), jnp.float32, low / len(cuts), top_value / len(cuts))
        factor_of = factor_of * jnp.repeat(jnp.exp(draws), shape[dim] // parts).reshape((-1,) + (1,) * (len(shape) - 1 - dim))
    return factor_of


def normal_values(stream_key, extent, width, bound, cuts=(), held_as=jnp.bfloat16):
    loudness = block_levels(stream_key, extent, cuts, -0.22, 0.18) if cuts else 1.0
    entries = jax.random.normal(stream_key, extent, jnp.float32) * width * loudness
    return jnp.minimum(jnp.maximum(entries, -bound), bound).astype(held_as)


def setup_inputs(seed: int = 0) -> dict:
    key_list = jax.random.split(jax.random.key(seed), 22)
    tokens = normal_values(key_list[0], (SEQ, D), 1.0, 6.0, ((0, 8),))
    input_gain = jnp.clip(1.0 + 0.18 * jax.random.normal(key_list[1], (D,), jnp.float32), 0.1, 1.9)
    chain_query = normal_values(key_list[2], (D, REC_KEYS), D ** -0.5, 0.125, ((0, 8), (1, 4)))
    forward_gate = normal_values(key_list[3], (D, REC_KEYS), D ** -0.5, 0.125, ((0, 8), (1, 4)))
    backward_gate = normal_values(key_list[4], (D, REC_KEYS), D ** -0.5, 0.125, ((0, 8), (1, 4)))
    chain_value = normal_values(key_list[5], (D, REC_WIDTH), D ** -0.5, 0.125, ((0, 8), (1, 4)))
    output_gate = normal_values(key_list[6], (D, REC_WIDTH), D ** -0.5, 0.125, ((0, 8), (1, 4)))
    forget_rate = jnp.clip(jnp.exp(math.log(6.0) - 3.4011974 * jax.random.uniform(key_list[7], (2, REC_KEYS), jnp.float32) ** block_levels(key_list[7], (2, REC_KEYS), ((1, 4),), -0.2, 0.2)), 0.2, 6.0)
    chain_gain = jnp.clip(1.0 + 0.18 * jax.random.normal(key_list[8], (REC_WIDTH,), jnp.float32), 0.1, 1.9)
    query_down = normal_values(key_list[9], (D, QLAT), D ** -0.5, 0.125, ((0, 8),))
    latent_down = normal_values(key_list[10], (D, KVLAT), D ** -0.5, 0.125, ((0, 8),))
    rotary_down = normal_values(key_list[11], (D, ROPE_DIM), D ** -0.5, 0.125)
    query_latent_gain = jnp.clip(1.0 + 0.18 * jax.random.normal(key_list[12], (QLAT,), jnp.float32), 0.1, 1.9)
    latent_gain = jnp.clip(1.0 + 0.18 * jax.random.normal(key_list[13], (KVLAT,), jnp.float32), 0.1, 1.9)
    query_up = normal_values(key_list[14], (QLAT, HEADS_ATT * ATT_QK), QLAT ** -0.5, 0.21875, ((1, 4),))
    latent_up = normal_values(key_list[15], (KVLAT, HEADS_ATT * (NOPE_DIM + VHEAD_DIM)), KVLAT ** -0.5, 0.25, ((1, 4),))
    query_head_gain = jnp.clip(1.0 + 0.18 * jax.random.normal(key_list[16], (ATT_QK,), jnp.float32), 0.1, 1.9)
    key_head_gain = jnp.clip(1.0 + 0.18 * jax.random.normal(key_list[17], (ATT_QK,), jnp.float32), 0.1, 1.9)
    mixer_gain = jnp.clip(1.0 + 0.18 * jax.random.normal(key_list[18], (ATT_WIDTH,), jnp.float32), 0.1, 1.9)
    chain_out = normal_values(key_list[19], (REC_WIDTH, D), (REC_WIDTH + ATT_WIDTH) ** -0.5, 0.125, ((0, 4), (1, 8)))
    attend_out = normal_values(key_list[20], (ATT_WIDTH, D), (REC_WIDTH + ATT_WIDTH) ** -0.5, 0.125, ((0, 4), (1, 8)))
    return dict(tokens=tokens, input_gain=input_gain, chain_query=chain_query, forward_gate=forward_gate, backward_gate=backward_gate, chain_value=chain_value, output_gate=output_gate, forget_rate=forget_rate, chain_gain=chain_gain, query_down=query_down, latent_down=latent_down, rotary_down=rotary_down, query_latent_gain=query_latent_gain, latent_gain=latent_gain, query_up=query_up, latent_up=latent_up, query_head_gain=query_head_gain, key_head_gain=key_head_gain, mixer_gain=mixer_gain, chain_out=chain_out, attend_out=attend_out)


norm_eps = 1e-06
rope_theta = 10000.0
finest_arithmetic_mode = lax.Precision.HIGHEST

def rms_scale(values, gain_vec):
    mean_square = lax.optimization_barrier(jnp.mean(values * values, axis=-1, keepdims=True))
    return values * lax.rsqrt(mean_square + norm_eps) * gain_vec

def rotate_tail(values, positions):
    half_dim = ROPE_DIM // 2
    inverse = rope_theta ** (-jnp.arange(0, ROPE_DIM, 2).astype(jnp.float32) / ROPE_DIM)
    angles = positions.astype(jnp.float32)[:, None] * inverse
    cosine = jnp.cos(angles)[:, None, :]
    sine_table = jnp.sin(angles)[:, None, :]
    unrotated = values[..., :NOPE_DIM]
    first_half = values[..., NOPE_DIM:NOPE_DIM + half_dim]
    latter_element = values[..., NOPE_DIM + half_dim:]
    return jnp.concatenate([unrotated, first_half * cosine - latter_element * sine_table, latter_element * cosine + first_half * sine_table], axis=-1)

def gate_parts(pre_gate, rate_row, seq_len):
    opening = rate_row / seq_len * jax.nn.sigmoid(-pre_gate.astype(jnp.float32))
    return (jnp.log1p(-opening), opening)

def summarize(query_rows, key_rows, payload_array_lines, log_decay):
    cumulative = jnp.cumsum(log_decay, axis=0)
    weighted_probe_vectors = query_rows * jnp.exp(cumulative)
    weighted_lookup_vectors = key_rows * jnp.exp(-cumulative)
    overall_shrink_multiplier = jnp.exp(cumulative[-1])
    recurrent_memory_digest = overall_shrink_multiplier[:, :, None] * jnp.einsum('jre,jrw->rew', weighted_lookup_vectors, payload_array_lines, precision=finest_arithmetic_mode)
    return (weighted_probe_vectors, weighted_lookup_vectors, overall_shrink_multiplier, recurrent_memory_digest)

def emit(weighted_probe_vectors, weighted_lookup_vectors, payload_array_lines, incoming_update):
    length = weighted_probe_vectors.shape[0]
    lower_mask = jnp.tril(jnp.ones((length, length), jnp.float32))
    scores = jnp.einsum('thk,shk->hts', weighted_probe_vectors, weighted_lookup_vectors, precision=finest_arithmetic_mode) * lower_mask
    within = jnp.einsum('hts,shv->thv', scores, payload_array_lines, precision=finest_arithmetic_mode)
    prior_state = jnp.einsum('mjf,jfi->mji', weighted_probe_vectors, incoming_update, precision=finest_arithmetic_mode)
    return within + prior_state

def run_chain(query_rows, key_rows, payload_array_lines, log_decay):
    seq_len, heads_here, key_dim = query_rows.shape
    blocks = seq_len // TOK_DEV

    def to_blocks(tensor):
        return tensor.reshape(blocks, TOK_DEV, heads_here, tensor.shape[2])

    def advance(carried, block_in):
        weighted_probe_vectors, weighted_lookup_vectors, overall_shrink_multiplier, recurrent_memory_digest = summarize(block_in[0], block_in[1], block_in[2], block_in[3])
        outputs = emit(weighted_probe_vectors, weighted_lookup_vectors, block_in[2], carried)
        return (overall_shrink_multiplier[:, :, None] * carried + recurrent_memory_digest, outputs)
    initial = jnp.zeros((heads_here, key_dim, payload_array_lines.shape[2]), jnp.float32)
    _, produced = lax.scan(advance, initial, (to_blocks(query_rows), to_blocks(key_rows), to_blocks(payload_array_lines), to_blocks(log_decay)))
    return produced.reshape(seq_len, heads_here, payload_array_lines.shape[2])

def reference(tokens, input_gain, chain_query, forward_gate, backward_gate, chain_value, output_gate, forget_rate, chain_gain, query_down, latent_down, rotary_down, query_latent_gain, latent_gain, query_up, latent_up, query_head_gain, key_head_gain, mixer_gain, chain_out, attend_out):
    seq_len = tokens.shape[0]
    normed = rms_scale(tokens.astype(jnp.float32), input_gain).astype(jnp.bfloat16)

    def project(source, weight):
        return jnp.dot(source, weight, preferred_element_type=jnp.float32).astype(jnp.bfloat16)

    def heads_of(tensor, head_width):
        return tensor.astype(jnp.float32).reshape(seq_len, tensor.shape[1] // head_width, head_width)
    query_rows = heads_of(project(normed, chain_query), KEY_DIM)
    payload_array_lines = heads_of(project(normed, chain_value), VAL_DIM)
    forward_log, forward_key = gate_parts(project(normed, forward_gate), forget_rate[0], seq_len)
    backward_log, backward_key = gate_parts(project(normed, backward_gate), forget_rate[1], seq_len)
    gate_logit = project(normed, output_gate).astype(jnp.float32)
    forward_out = run_chain(query_rows, heads_of(forward_key, KEY_DIM), payload_array_lines, heads_of(forward_log, KEY_DIM))
    reversed_out = run_chain(jnp.flip(query_rows, 0), jnp.flip(heads_of(backward_key, KEY_DIM), 0), jnp.flip(payload_array_lines, 0), jnp.flip(heads_of(backward_log, KEY_DIM), 0))
    combined = forward_out + jnp.flip(reversed_out, 0)
    head_gain = chain_gain.reshape(combined.shape[1], VAL_DIM)
    chain_mixed = (rms_scale(combined, head_gain).reshape(seq_len, -1) * jax.nn.silu(gate_logit)).astype(jnp.bfloat16)
    query_latent = rms_scale(project(normed, query_down).astype(jnp.float32), query_latent_gain).astype(jnp.bfloat16)
    pair_latent = rms_scale(project(normed, latent_down).astype(jnp.float32), latent_gain).astype(jnp.bfloat16)
    rotary_key = project(normed, rotary_down).astype(jnp.float32)
    attend_query = project(query_latent, query_up).astype(jnp.float32).reshape(seq_len, HEADS_ATT, ATT_QK)
    attend_pairs = project(pair_latent, latent_up).reshape(seq_len, HEADS_ATT, NOPE_DIM + VHEAD_DIM)
    positions = jnp.arange(seq_len, dtype=jnp.int32)
    query_final = rotate_tail(rms_scale(attend_query, query_head_gain), positions).astype(jnp.bfloat16)
    key_cat = jnp.concatenate([attend_pairs[..., :NOPE_DIM].astype(jnp.float32), jnp.broadcast_to(rotary_key[:, None, :], (seq_len, HEADS_ATT, ROPE_DIM))], axis=-1)
    key_final = rotate_tail(rms_scale(key_cat, key_head_gain), positions).astype(jnp.bfloat16)
    key_wide = key_final.astype(jnp.float32)
    value_wide = attend_pairs[..., NOPE_DIM:].astype(jnp.float32)
    score_scale = ATT_QK ** (-0.5)

    def attend(query_block):
        scores = jnp.einsum('qhd,khd->hqk', query_block.astype(jnp.float32), key_wide) * score_scale
        weights = jnp.exp(scores)
        rounded = lax.optimization_barrier(weights.astype(jnp.bfloat16)).astype(jnp.float32)
        numerator = jnp.einsum('hqk,khv->qhv', rounded, value_wide)
        return numerator / jnp.transpose(lax.optimization_barrier(jnp.sum(weights, axis=-1)))[:, :, None]
    blocks_in = query_final.reshape(seq_len // TOK_DEV, TOK_DEV, HEADS_ATT, ATT_QK)
    attend_rows = lax.map(attend, blocks_in).reshape(seq_len, HEADS_ATT, VHEAD_DIM)
    attend_mixed = rms_scale(attend_rows, mixer_gain.reshape(HEADS_ATT, VHEAD_DIM)).reshape(seq_len, ATT_WIDTH).astype(jnp.bfloat16)
    mixed_sum = jnp.dot(chain_mixed, chain_out, preferred_element_type=jnp.float32) + jnp.dot(attend_mixed, attend_out, preferred_element_type=jnp.float32)
    return mixed_sum
```

```python
import functools

import jax
import jax.numpy as jnp
import numpy as np
from jax import lax
from jax.experimental import pallas as pl
from jax.experimental.pallas import tpu as pltpu
from jax.sharding import PartitionSpec as P

LANES = 128
NOPE_DIM = 128
ROPE_DIM = 64
ATT_QK = 192
HALF = ROPE_DIM // 2

norm_eps = 1e-06
rope_theta = 10000.0
MESH = pl.DeviceIdType.MESH
VMEM_LIMIT = 60 * 1024 * 1024
f32 = jnp.float32
bf16 = jnp.bfloat16


def run_if(condition, act):
    if condition is None:
        act()
    else:
        pl.when(condition)(act)


def both(a, b):
    if a is None:
        return b
    if b is None:
        return a
    return jnp.logical_and(a, b)


def against(a, b):
    return lax.dot_general(a, b, (((1,), (1,)), ((), ())), preferred_element_type=f32)


def inverse_rms(values, size):
    return lax.rsqrt(jnp.sum(values * values, axis=-1, keepdims=True) / size + norm_eps)


def spread(count, start, signed):
    row = lax.broadcasted_iota(jnp.int32, (count, 3 * LANES), 0) - start
    col = lax.broadcasted_iota(jnp.int32, (count, 3 * LANES), 1)
    straight = (col < ATT_QK) & (row == col)
    at = col - 2 * LANES
    low = (at >= 0) & (at < HALF) & (row == NOPE_DIM + HALF + at)
    high = (at >= HALF) & (at < ROPE_DIM) & (row == NOPE_DIM + at - HALF)
    return (
        jnp.where(straight, 1.0, 0.0)
        + jnp.where(low, -1.0 if signed else 1.0, 0.0)
        + jnp.where(high, 1.0, 0.0)
    )


def mixer_kernel(n, heads_n, heads, sends, *refs):
    (
        tok_in,
        wv,
        wf,
        wb,
        wq,
        wg,
        q_down,
        l_down,
        rot_down,
        query_up,
        latent_up,
        chain_out,
        attend_out,
        rate_in,
        chain_gain_in,
        mixer_gain_in,
        input_gain,
        query_latent_gain,
        latent_gain,
        query_gain,
        key_gain,
        cos_row,
        sin_row,
        cos_block,
        sin_block,
        out_ref,
        stage,
        tok,
        xs,
        w_all,
        l_all,
        rot_all,
        lat,
        rate_ref,
        chain_gain_ref,
        mixer_gain_ref,
        up_q,
        up_l,
        kv,
        states,
        logs,
        mix_send,
        mix_recv,
        out_w,
        send,
        recv,
        ssem,
        r_tok,
        r_deliver,
        r_lat_w,
        r_rec_w,
        r_small,
        r_lat,
        r_kv,
        r_state,
        r_log,
        r_mix,
        r_out,
        r_sum,
    ) = refs
    mats = (wv, wf, wb, wq, wg)
    groups = ((0, 3), (3, 2))
    outer_n = 2 * heads
    inner_n = n // outer_n
    blocks = outer_n // 2
    part_rows, width = tok_in.shape[1:]
    rows = part_rows * heads_n
    q_units = q_down.shape[2] // LANES

    me = lax.axis_index("sp")
    t = lax.axis_index("tp")
    o, i = me // inner_n, lax.rem(me, inner_n)
    x, k = t // 2, lax.rem(t, 2)
    other = 1 - k
    at_home = (o // heads) == k
    away = jnp.logical_not(at_home)
    hh = lax.rem(o, heads)

    def dev(o_, i_, x_, k_):
        return {"sp": o_ * inner_n + i_, "tp": x_ * 2 + k_}

    def turn_o(d):
        return lax.rem(o + d, outer_n)

    def turn_i(d):
        return lax.rem(i + d, inner_n)

    def lane(index, size=LANES):
        return pl.ds(pl.multiple_of(index * size, LANES), size)

    peers = [dev(turn_o(d), i, x, r) for d in range(1, outer_n) for r in range(2)]
    peers += [dev(o, turn_i(d), x, k) for d in range(1, inner_n)]
    peers += [{"sp": me, "tp": lax.rem(t + d, heads_n)} for d in range(1, heads_n)]
    barrier = pltpu.get_barrier_semaphore()
    for peer in peers:
        pl.semaphore_signal(barrier, inc=1, device_id=peer, device_id_type=MESH)
    pl.semaphore_wait(barrier, len(peers))

    pending = []

    def copy(src, dst, send_sem, recv_sem, device):
        return pltpu.make_async_remote_copy(
            src_ref=src,
            dst_ref=dst,
            send_sem=send_sem,
            recv_sem=recv_sem,
            device_id=device,
            device_id_type=MESH,
        )

    def launch(src, dst, recv_sem, device, condition=None):
        index = len(pending)
        assert index < sends

        def make():
            return copy(src, dst, ssem.at[index], recv_sem, device)

        run_if(condition, lambda: make().start())
        pending.append((condition, lambda: make().wait_send()))

    def arrive(dst, recv_sem, condition=None):
        run_if(
            condition,
            lambda: copy(dst, dst, ssem.at[0], recv_sem, dev(o, i, x, other)).wait_recv(),
        )

    partner = dev(o, i, x, other)
    beside = dev(o, i, 1 - x, k)

    right, left = o + 1 < outer_n, o > 0
    launch(tok_in.at[t], stage.at[o], r_tok.at[o], dev(o + 1, i, x, k), right)
    launch(tok_in.at[t], stage.at[o], r_tok.at[o], dev(o - 1, i, x, k), left)

    is_q, is_l = x == 0, x != 0
    extra_o, extra_unit = 1 + x, outer_n + x
    extra = o == extra_o
    for d in range(1, outer_n):
        there = turn_o(d)
        for source, condition in ((q_down, is_q), (l_down, is_l)):
            launch(
                source.at[k, :, lane(there)],
                l_all.at[0, me, k],
                r_lat_w.at[0, me, k],
                dev(there, i, x, k),
                condition,
            )
    launch(
        q_down.at[k, :, lane(extra_unit)],
        l_all.at[1, me, k],
        r_lat_w.at[1, me, k],
        dev(extra_o, i, x, k),
        jnp.logical_not(extra),
    )

    def send_weights(g):
        first, count = groups[g]
        for m in range(first, first + count):
            for h in range(heads):
                there = heads * k + h
                for r in range(2):
                    launch(
                        mats[m].at[r, :, h * LANES : (h + 1) * LANES],
                        w_all.at[me, m, r],
                        r_rec_w.at[g, me, r],
                        dev(there, i, x, r),
                        jnp.logical_not((there == o) & (k == r)),
                    )

    for j, (source, target) in enumerate(
        (
            (query_up, up_q),
            (latent_up.at[:, lane(hh, 2 * LANES)], up_l),
            (rate_in, rate_ref),
            (chain_gain_in, chain_gain_ref),
            (mixer_gain_in, mixer_gain_ref),
        )
    ):
        launch(source, target, r_small.at[j], partner, at_home)
    send_weights(0)

    @pl.when(is_q)
    def _():
        l_all[0, me, k] = q_down[k, :, lane(o)]

    @pl.when(is_l)
    def _():
        l_all[0, me, k] = l_down[k, :, lane(o)]

    @pl.when(extra)
    def _():
        l_all[1, me, k] = q_down[k, :, lane(extra_unit)]

    @pl.when(at_home)
    def _():
        for m in range(len(mats)):
            w_all[me, m, k] = mats[m][k, :, lane(hh)]
        up_q[...] = query_up[...]
        up_l[...] = latent_up[:, lane(hh, 2 * LANES)]
        rate_ref[...] = rate_in[...]
        chain_gain_ref[...] = chain_gain_in[...]
        mixer_gain_ref[...] = mixer_gain_in[...]

    def lat_piece(slot, s, half):
        return l_all.at[slot, s, half], r_lat_w.at[slot, s, half]

    def rec_piece(g, s, half):
        first, count = groups[g]
        return w_all.at[s, first : first + count, half], r_rec_w.at[g, s, half]

    def pass_on(piece, s, condition=None):
        ref, sem = piece(s, k)
        for e in range(1, inner_n):
            launch(ref, ref, sem, dev(o, turn_i(e), x, k), condition)
        launch(ref, ref, sem, partner, condition)

    def from_lines(piece, first, condition=None, own=None):
        for d in range(first, outer_n):
            s = turn_o(d) * inner_n + i
            wait = condition if d else own
            if d or own is not None:
                arrive(*piece(s, k), wait)
            pass_on(piece, s, condition)

    def from_pairs(piece, condition=None):
        for e in range(1, inner_n):
            for d in range(outer_n):
                s = turn_o(d) * inner_n + turn_i(e)
                ref, sem = piece(s, k)
                arrive(ref, sem, condition)
                launch(ref, ref, sem, partner, condition)

    def from_partner(piece, condition=None):
        def wait_all():
            @pl.loop(0, n)
            def _(s):
                arrive(*piece(s, other))

        run_if(condition, wait_all)

    lat_a = functools.partial(lat_piece, 0)
    lat_b = functools.partial(lat_piece, 1)
    rec = [functools.partial(rec_piece, g) for g in range(2)]

    def own_line(piece, condition=None, own=None):
        if own is not None:
            arrive(*piece(me, k), own)
        pass_on(piece, me, condition)

    own_line(lat_a)
    own_line(lat_b, extra)

    for b in range(blocks):

        @pl.when(blocks * k + b == o)
        def _():
            tok[b] = tok_in[...]

    sign_pick = spread(ATT_QK, 0, True)[NOPE_DIM:, LANES:].astype(bf16)

    @pl.loop(0, n)
    def _(s):
        rot_all[s] = jnp.dot(rot_down[s], sign_pick, preferred_element_type=f32).astype(bf16)

    own_line(rec[0], None, away)

    def gains(ref):
        wide = jnp.broadcast_to(ref[...], (8, ATT_QK))
        return jnp.dot(
            wide,
            spread(ATT_QK, 0, False),
            precision=lax.Precision.HIGHEST,
            preferred_element_type=f32,
        )[0:1]

    for j, target in enumerate((up_q, up_l, rate_ref, chain_gain_ref, mixer_gain_ref)):
        arrive(target, r_small.at[j], away)
    up_q[...] = jnp.dot(
        up_q[...],
        spread(heads * ATT_QK, hh * ATT_QK, True).astype(bf16),
        preferred_element_type=f32,
    ).astype(bf16)

    def deliver(there, condition):
        core, b = there // blocks, lax.rem(there, blocks)
        launch(
            stage.at[there], tok.at[b, t], r_deliver.at[b, t], dev(o, i, 1 - x, core), condition
        )
        launch(
            stage.at[there],
            tok.at[b, t],
            r_deliver.at[b, t],
            partner,
            both(condition, core != k),
        )

        @pl.when(both(condition, core == k))
        def _():
            tok[b, t] = stage[there]

    for d in range(1, outer_n):
        for there, onward, step in ((o - d, right, 1), (o + d, left, -1)):
            valid = (there >= 0) & (there < outer_n)
            there = jnp.clip(there, 0, outer_n - 1)
            arrive(stage.at[there], r_tok.at[there], valid)
            launch(
                stage.at[there],
                stage.at[there],
                r_tok.at[there],
                dev(o + step, i, x, k),
                both(valid, onward),
            )
            deliver(there, valid)

    from_lines(lat_a, 1)
    from_lines(lat_b, 1, extra)
    from_pairs(lat_a)
    from_pairs(lat_b, extra)

    depth = width // n
    for b in range(blocks):
        there = blocks * k + b
        for d in range(1, heads_n):
            q = lax.rem(t + d, heads_n)
            arrive(tok.at[b, q], r_deliver.at[b, q], there != o)
        wide = jnp.concatenate([tok[b, q].astype(f32) for q in range(heads_n)], axis=0)
        scale = inverse_rms(wide, width)
        normed = (wide * scale * input_gain[...]).astype(bf16)
        for s in range(n):
            xs[s, b * rows : (b + 1) * rows, :] = normed[:, s * depth : (s + 1) * depth]

    def project(rhs, columns):
        def body(s, total):
            return total + jnp.dot(xs[s], rhs(s), preferred_element_type=f32)

        return lax.fori_loop(
            0, n, body, jnp.zeros((blocks * rows, columns), f32), unroll=n <= 8
        ).astype(bf16)

    from_partner(lat_a)
    from_partner(lat_b, extra)
    own_unit = x * q_units + o
    first = project(
        lambda s: jnp.concatenate([l_all[0, s].reshape(depth, LANES), rot_all[s]], axis=1),
        3 * LANES,
    )
    lat[own_unit] = first[:, :LANES]
    rotary = first[:, LANES:].astype(f32)

    @pl.when(extra)
    def _():
        lat[extra_unit] = project(lambda s: l_all[1, s].reshape(depth, LANES), LANES)

    def send_unit(unit, condition=None):
        for d in range(1, outer_n):
            launch(lat.at[unit], lat.at[unit], r_lat.at[unit], dev(turn_o(d), i, x, k), condition)
        launch(lat.at[unit], lat.at[unit], r_lat.at[unit], beside, condition)

    send_unit(own_unit)
    send_unit(extra_unit, extra)
    send_weights(1)

    def out_piece(j, s):
        return out_w.at[j, s], r_out.at[j, s]

    outs = (chain_out, attend_out)
    for j in range(2):
        for d in range(1, outer_n):
            ref, sem = out_piece(j, me)
            launch(outs[j], ref, sem, dev(turn_o(d), i, x, k))
        out_w[j, me] = outs[j][...]

    from_lines(rec[0], 1)

    def relay_unit(unit, condition=None):
        arrive(lat.at[unit], r_lat.at[unit], condition)
        launch(lat.at[unit], lat.at[unit], r_lat.at[unit], beside, condition)

    for d in range(1, outer_n):
        relay_unit(x * q_units + turn_o(d))
    relay_unit(extra_unit, jnp.logical_not(extra))
    from_pairs(rec[0])

    for d in range(outer_n):
        unit = (1 - x) * q_units + turn_o(d)
        arrive(lat.at[unit], r_lat.at[unit])
    far_unit = outer_n + 1 - x
    arrive(lat.at[far_unit], r_lat.at[far_unit])

    cosines, sines = [], []
    for b in range(blocks):
        s = (blocks * k + b) * inner_n + i
        cb, sb = cos_block[pl.ds(s, 1), :], sin_block[pl.ds(s, 1), :]
        cosines.append(cb * cos_row[...] - sb * sin_row[...])
        sines.append(sb * cos_row[...] + cb * sin_row[...])
    cosine = jnp.concatenate(cosines, axis=0)
    sine = jnp.concatenate(sines, axis=0)

    def latent(first_unit, count, gain):
        wide = jnp.concatenate(
            [lat[u].astype(f32) for u in range(first_unit, first_unit + count)], axis=1
        )
        return (wide * inverse_rms(wide, count * LANES) * gain[...]).astype(bf16)

    def finish(plain, tail, swapped, gain):
        square = jnp.sum(plain * plain + tail * tail, axis=-1, keepdims=True)
        scale = lax.rsqrt(square / ATT_QK + norm_eps)
        turned = tail * gain[:, LANES : 2 * LANES] * cosine + swapped * gain[:, 2 * LANES :] * sine
        return jnp.concatenate(
            [(plain * scale * gain[:, :LANES]).astype(bf16), (turned * scale).astype(bf16)], axis=1
        )

    pairs = jnp.dot(
        latent(q_units, outer_n, latent_gain), up_l[...], preferred_element_type=f32
    ).astype(bf16)
    kv[i, k, :, : 2 * LANES] = finish(
        pairs[:, :LANES].astype(f32), rotary[:, :LANES], rotary[:, LANES:], gains(key_gain)
    )
    kv[i, k, :, 2 * LANES :] = pairs[:, LANES:]

    def shared(ref, sem):
        for e in range(1, inner_n):
            launch(ref, ref, sem, dev(o, turn_i(e), x, k))
        launch(ref, ref, sem, partner)

    shared(kv.at[i, k], r_kv.at[i, k])

    attend_q = (
        jnp.dot(latent(0, q_units, query_latent_gain), up_q[...], preferred_element_type=f32)
        .astype(bf16)
        .astype(f32)
    )
    query = finish(
        attend_q[:, :LANES],
        attend_q[:, LANES : 2 * LANES],
        attend_q[:, 2 * LANES :],
        gains(query_gain),
    )

    def columns(s, mats_here):
        return jnp.concatenate([w_all[s, m].reshape(depth, LANES) for m in mats_here], axis=1)

    from_partner(rec[0])
    vfb = project(lambda s: columns(s, (0, 1, 2)), 3 * LANES)
    value = [vfb[b * rows : (b + 1) * rows, :LANES] for b in range(blocks)]
    row = lax.broadcasted_iota(jnp.int32, (rows, rows), 0)
    col = lax.broadcasted_iota(jnp.int32, (rows, rows), 1)
    masks = (row >= col, row <= col)

    def direction(d):
        rate = rate_ref[d : d + 1, lane(hh)] / (rows * n)
        logit = vfb[:, (1 + d) * LANES : (2 + d) * LANES].astype(f32)
        key = rate * jax.nn.sigmoid(-logit)
        decay = jnp.log1p(-key)
        total = jnp.dot(
            jnp.where(masks[d], 1.0, 0.0),
            jnp.concatenate([decay[b * rows : (b + 1) * rows] for b in range(blocks)], axis=1),
            precision=lax.Precision.HIGHEST,
            preferred_element_type=f32,
        )
        keys, totals = [], []
        last = (rows - 1, 0)[d]
        for b in range(blocks):
            part = total[:, b * LANES : (b + 1) * LANES]
            full = part[last : last + 1, :]
            near = (key[b * rows : (b + 1) * rows] * jnp.exp(-part)).astype(bf16)
            state = lax.dot_general(
                value[b], near, (((0,), (0,)), ((), ())), preferred_element_type=f32
            )
            states[i, blocks * k + b, d] = (state * jnp.exp(full)).astype(bf16)
            logs[i, blocks * k + b, d] = jnp.broadcast_to(full, (8, LANES))
            keys.append(near)
            totals.append(part)
        return keys, totals

    near = [direction(d) for d in range(2)]

    def state_pieces(i_, k_):
        at = pl.ds(k_ * blocks, blocks)
        return (states.at[i_, at], r_state.at[i_, k_]), (logs.at[i_, at], r_log.at[i_, k_])

    for ref, sem in state_pieces(i, k):
        shared(ref, sem)

    own_line(rec[1], None, away)
    from_lines(rec[1], 1)
    for j in range(2):
        ref, sem = out_piece(j, me)
        for e in range(1, inner_n):
            launch(outs[j], ref, sem, dev(o, turn_i(e), x, k))

    scale = ATT_QK ** (-0.5) * 1.4426950408889634

    def attend(carry, i_, k_):
        numer, denom = carry
        score = against(query, kv[i_, k_, :, : 2 * LANES])
        weight = jnp.exp2(score * scale)
        numer += jnp.dot(
            weight.astype(bf16), kv[i_, k_, :, 2 * LANES :], preferred_element_type=f32
        )
        return numer, denom + jnp.sum(weight, axis=-1, keepdims=True)

    carry = (jnp.zeros((blocks * rows, LANES), f32), jnp.zeros((blocks * rows, 1), f32))
    carry = attend(carry, i, k)
    arrive(kv.at[i, other], r_kv.at[i, other])
    carry = attend(carry, i, other)

    def relay_pair(ref, sem):
        arrive(ref, sem)
        launch(ref, ref, sem, partner)

    for e in range(1, inner_n):
        relay_pair(kv.at[turn_i(e), k], r_kv.at[turn_i(e), k])
    for e in range(1, inner_n):
        for ref, sem in state_pieces(turn_i(e), k):
            relay_pair(ref, sem)
    from_pairs(rec[1])
    for e in range(1, inner_n):
        there = turn_i(e)
        carry = attend(carry, there, k)
        arrive(kv.at[there, other], r_kv.at[there, other])
        carry = attend(carry, there, other)
    rows_out = carry[0] / carry[1]
    attend_mixed = (
        rows_out * inverse_rms(rows_out, LANES) * mixer_gain_ref[:, lane(hh)]
    ).astype(bf16)

    for j in range(2):
        for d in range(1, outer_n):
            s = turn_o(d) * inner_n + i
            ref, sem = out_piece(j, s)
            arrive(ref, sem)
            for e in range(1, inner_n):
                launch(ref, ref, sem, dev(o, turn_i(e), x, k))

    from_partner(rec[1])
    qg = project(lambda s: columns(s, (3, 4)), 2 * LANES).astype(f32)
    for e in range(inner_n):
        for k_ in (k, other):
            if e or k_ is other:
                for ref, sem in state_pieces(turn_i(e), k_):
                    if k_ is other:
                        arrive(ref, sem)

    def forward(s, state):
        i_, o_ = lax.rem(s, inner_n), s // inner_n
        return state * jnp.exp(logs[i_, o_, 0, 0:1, :]) + states[i_, o_, 0].astype(f32)

    def backward(j, state):
        s = n - 1 - j
        i_, o_ = lax.rem(s, inner_n), s // inner_n
        return state * jnp.exp(logs[i_, o_, 1, 0:1, :]) + states[i_, o_, 1].astype(f32)

    nothing = jnp.zeros((LANES, LANES), f32)
    for b in range(blocks):
        there = blocks * k + b
        s = there * inner_n + i
        incoming = (
            lax.fori_loop(0, s, forward, nothing).astype(bf16),
            lax.fori_loop(0, n - 1 - s, backward, nothing).astype(bf16),
        )
        at = slice(b * rows, (b + 1) * rows)
        total = jnp.zeros((rows, LANES), f32)
        within = jnp.zeros((rows, rows), f32)
        for d in range(2):
            keys, totals = near[d]
            probe = (qg[at, :LANES] * jnp.exp(totals[b])).astype(bf16)
            within += jnp.where(masks[d], against(probe, keys[b]), 0.0)
            total += against(probe, incoming[d])
        total += jnp.dot(within.astype(bf16), value[b], preferred_element_type=f32)
        gate = qg[at, LANES:]
        scaled = total * inverse_rms(total, LANES) * chain_gain_ref[:, lane(hh)]
        mix_send[b, :, :LANES] = (scaled * (gate * jax.nn.sigmoid(gate))).astype(bf16)
        mix_send[b, :, LANES:] = attend_mixed[at]
        home = there == o
        launch(
            mix_send.at[b],
            mix_recv.at[hh],
            r_mix.at[hh],
            dev(there, i, x, o // heads),
            jnp.logical_not(home),
        )

        @pl.when(home)
        def _():
            mix_recv[hh] = mix_send[b]

    for j in range(2):
        for e in range(1, inner_n):
            for d in range(outer_n):
                arrive(*out_piece(j, turn_o(d) * inner_n + turn_i(e)))
    for h in range(heads):
        arrive(mix_recv.at[h], r_mix.at[h], heads * k + h != o)
    chain_mixed = jnp.concatenate([mix_recv[h, :, :LANES] for h in range(heads)], axis=1)
    attended = jnp.concatenate([mix_recv[h, :, LANES:] for h in range(heads)], axis=1)
    col_n = out_w.shape[3]
    for s in range(n):
        product = jnp.dot(chain_mixed, out_w[0, s], preferred_element_type=f32) + jnp.dot(
            attended, out_w[1, s], preferred_element_type=f32
        )
        for q in range(heads_n):
            send[q, :, s * col_n : (s + 1) * col_n] = product[
                q * part_rows : (q + 1) * part_rows
            ].astype(bf16)
    for d in range(1, heads_n):
        there = lax.rem(t + d, heads_n)
        launch(send.at[there], recv.at[d], r_sum.at[d], {"sp": me, "tp": there})
    total = send[t].astype(f32)
    for d in range(1, heads_n):
        arrive(recv.at[d], r_sum.at[d])
        total = total + recv[d].astype(f32)
    out_ref[...] = total
    for condition, finish_send in pending:
        run_if(condition, finish_send)


def on_device(
    tokens,
    input_gain,
    chain_query,
    forward_gate,
    backward_gate,
    chain_value,
    output_gate,
    forget_rate,
    chain_gain,
    query_down,
    latent_down,
    rotary_down,
    query_latent_gain,
    latent_gain,
    query_up,
    latent_up,
    query_head_gain,
    key_head_gain,
    mixer_gain,
    chain_out,
    attend_out,
):
    n, heads_n = lax.axis_size("sp"), lax.axis_size("tp")
    rows, width = tokens.shape
    depth = chain_query.shape[0]
    heads = query_up.shape[1] // ATT_QK
    outer_n = 2 * heads
    inner_n = n // outer_n
    blocks = outer_n // 2
    half = depth // 2
    units = (query_down.shape[1] + latent_down.shape[1]) // LANES
    part = rows // heads_n
    out_cols = n * chain_out.shape[1]

    inverse = rope_theta ** (-np.arange(0, ROPE_DIM, 2) / ROPE_DIM)

    def table(positions):
        angles = np.tile(positions[:, None] * inverse, (1, 2))
        pad = ((0, 0), (0, LANES - ROPE_DIM))
        return [jnp.asarray(np.pad(f(angles), pad), f32) for f in (np.cos, np.sin)]

    in_row = table(np.arange(rows, dtype=np.float64))
    in_block = table(np.arange(n, dtype=np.float64) * rows)

    def halves(w):
        return w.reshape(2, half, w.shape[1])

    operands = (
        tokens.reshape(heads_n, part, width),
        *[
            halves(w)
            for w in (
                chain_value,
                forward_gate,
                backward_gate,
                chain_query,
                output_gate,
                query_down,
                latent_down,
            )
        ],
        rotary_down.reshape(n, depth, ROPE_DIM),
        query_up,
        latent_up,
        chain_out,
        attend_out,
        forget_rate,
        chain_gain[None],
        mixer_gain[None],
        input_gain[None],
        query_latent_gain[None],
        latent_gain[None],
        query_head_gain[None],
        key_head_gain[None],
        *in_row,
        *in_block,
    )
    sends = 120 + 26 * n
    dma = pltpu.SemaphoreType.DMA
    vmem = pl.BlockSpec(memory_space=pltpu.VMEM)
    tall = blocks * rows
    return pl.pallas_call(
        functools.partial(mixer_kernel, n, heads_n, heads, sends),
        out_shape=jax.ShapeDtypeStruct((part, out_cols), f32),
        in_specs=[vmem] * len(operands),
        out_specs=vmem,
        scratch_shapes=[
            pltpu.VMEM((outer_n, part, width), bf16),
            pltpu.VMEM((blocks, heads_n, part, width), bf16),
            pltpu.VMEM((n, tall, depth), bf16),
            pltpu.VMEM((n, 5, 2, half, LANES), bf16),
            pltpu.VMEM((2, n, 2, half, LANES), bf16),
            pltpu.VMEM((n, depth, 2 * LANES), bf16),
            pltpu.VMEM((units, tall, LANES), bf16),
            pltpu.VMEM(forget_rate.shape, f32),
            pltpu.VMEM((1,) + chain_gain.shape, f32),
            pltpu.VMEM((1,) + mixer_gain.shape, f32),
            pltpu.VMEM(query_up.shape, bf16),
            pltpu.VMEM((latent_up.shape[0], 2 * LANES), bf16),
            pltpu.VMEM((inner_n, 2, tall, 3 * LANES), bf16),
            pltpu.VMEM((inner_n, outer_n, 2, LANES, LANES), bf16),
            pltpu.VMEM((inner_n, outer_n, 2, 8, LANES), f32),
            pltpu.VMEM((blocks, rows, 2 * LANES), bf16),
            pltpu.VMEM((heads, rows, 2 * LANES), bf16),
            pltpu.VMEM((2, n) + chain_out.shape, bf16),
            pltpu.VMEM((heads_n, part, out_cols), bf16),
            pltpu.VMEM((heads_n, part, out_cols), bf16),
            dma((sends,)),
            dma((outer_n,)),
            dma((blocks, heads_n)),
            dma((2, n, 2)),
            dma((2, n, 2)),
            dma((5,)),
            dma((units,)),
            dma((inner_n, 2)),
            dma((inner_n, 2)),
            dma((inner_n, 2)),
            dma((heads,)),
            dma((2, n)),
            dma((heads_n,)),
        ],
        compiler_params=pltpu.CompilerParams(
            collective_id=0, has_side_effects=True, vmem_limit_bytes=VMEM_LIMIT
        ),
    )(*operands)


def solution(mesh):
    placed = (
        P("sp", None),
        P(),
        P("sp", "tp"),
        P("sp", "tp"),
        P("sp", "tp"),
        P("sp", "tp"),
        P("sp", "tp"),
        P(None, "tp"),
        P("tp"),
        P("sp", None),
        P("sp", None),
        P(),
        P(),
        P(),
        P(None, "tp"),
        P(None, "tp"),
        P(),
        P(),
        P("tp"),
        P("tp", "sp"),
        P("tp", "sp"),
    )
    return jax.shard_map(
        on_device, mesh=mesh, in_specs=placed, out_specs=P(("sp", "tp"), None), check_vma=False
    )
```

```python
import functools

import jax
import jax.numpy as jnp
import numpy as np
from jax import lax
from jax.experimental import pallas as pl
from jax.experimental.pallas import tpu as pltpu
from jax.sharding import PartitionSpec as P

LANES = 128
NOPE_DIM = 128
ROPE_DIM = 64
ATT_QK = 192
HALF = ROPE_DIM // 2

norm_eps = 1e-06
rope_theta = 10000.0
MESH = pl.DeviceIdType.MESH
VMEM_LIMIT = 60 * 1024 * 1024
f32 = jnp.float32
bf16 = jnp.bfloat16


def run_if(condition, act):
    if condition is None:
        act()
    else:
        pl.when(condition)(act)


def both(a, b):
    if a is None:
        return b
    if b is None:
        return a
    return jnp.logical_and(a, b)


def against(a, b):
    return lax.dot_general(a, b, (((1,), (1,)), ((), ())), preferred_element_type=f32)


def inverse_rms(values, size):
    return lax.rsqrt(jnp.sum(values * values, axis=-1, keepdims=True) / size + norm_eps)


def spread(count, start, signed):
    row = lax.broadcasted_iota(jnp.int32, (count, 3 * LANES), 0) - start
    col = lax.broadcasted_iota(jnp.int32, (count, 3 * LANES), 1)
    straight = (col < ATT_QK) & (row == col)
    at = col - 2 * LANES
    low = (at >= 0) & (at < HALF) & (row == NOPE_DIM + HALF + at)
    high = (at >= HALF) & (at < ROPE_DIM) & (row == NOPE_DIM + at - HALF)
    return (
        jnp.where(straight, 1.0, 0.0)
        + jnp.where(low, -1.0 if signed else 1.0, 0.0)
        + jnp.where(high, 1.0, 0.0)
    )


def mixer_kernel(n, heads_n, heads, sends, needed, *refs):
    count = 13
    far, near_by = refs[:count], refs[-count - 1 : -1]
    fetched = refs[-1]
    (
        tok_in,
        wv,
        wf,
        wb,
        wq,
        wg,
        q_down,
        l_down,
        rot_down,
        query_up,
        latent_up,
        chain_out,
        attend_out,
    ) = near_by
    (
        rate_in,
        chain_gain_in,
        mixer_gain_in,
        input_gain,
        query_latent_gain,
        latent_gain,
        query_gain,
        key_gain,
        cos_row,
        sin_row,
        cos_block,
        sin_block,
        out_ref,
        stage,
        tok,
        xs,
        w_all,
        l_all,
        rot_all,
        lat,
        rate_ref,
        chain_gain_ref,
        mixer_gain_ref,
        up_q,
        up_l,
        kv,
        states,
        logs,
        mix_send,
        mix_recv,
        out_w,
        part_far,
        part_near,
        send_far,
        send_near,
        got_far,
        got_near,
        send_x,
        got_x,
        ssem,
        r_tok,
        r_deliver,
        r_lat_w,
        r_lat_p,
        r_rec_w,
        r_rec_p,
        r_small,
        r_lat,
        r_kv,
        r_state,
        r_log,
        r_mix,
        r_out,
        r_sum,
    ) = refs[count : -count - 1]
    mats = (wv, wf, wb, wq, wg)
    groups = ((0, 3), (3, 2))
    outer_n = 2 * heads
    inner_n = n // outer_n
    blocks = outer_n // 2
    part_rows, width = tok_in.shape[1:]
    chunk = width // 2
    rows = part_rows * heads_n
    q_units = q_down.shape[2] // LANES

    me = lax.axis_index("sp")
    t = lax.axis_index("tp")
    o, i = me // inner_n, lax.rem(me, inner_n)
    x, k = t // 2, lax.rem(t, 2)
    other = 1 - k
    at_home = (o // heads) == k
    away = jnp.logical_not(at_home)
    hh = lax.rem(o, heads)

    def dev(o_, i_, x_, k_):
        return {"sp": o_ * inner_n + i_, "tp": x_ * 2 + k_}

    def turn_o(d):
        return lax.rem(o + d, outer_n)

    def turn_i(d):
        return lax.rem(i + d, inner_n)

    def lane(index, size=LANES):
        return pl.ds(pl.multiple_of(index * size, LANES), size)

    peers = [dev(turn_o(d), i, x, r) for d in range(1, outer_n) for r in range(2)]
    peers += [dev(o, turn_i(d), x, k) for d in range(1, inner_n)]
    peers += [{"sp": me, "tp": lax.rem(t + d, heads_n)} for d in range(1, heads_n)]
    fetches = [pltpu.make_async_copy(far[j], near_by[j], fetched.at[j]) for j in range(count)]
    for fetch in fetches:
        fetch.start()
    barrier = pltpu.get_barrier_semaphore()
    for peer in peers:
        pl.semaphore_signal(barrier, inc=1, device_id=peer, device_id_type=MESH)
    pl.semaphore_wait(barrier, len(peers))

    pending, spare, used = [], [], [0]

    def copy(src, dst, send_sem, recv_sem, device):
        return pltpu.make_async_remote_copy(
            src_ref=src,
            dst_ref=dst,
            send_sem=send_sem,
            recv_sem=recv_sem,
            device_id=device,
            device_id_type=MESH,
        )

    def launch(src, dst, recv_sem, device, condition=None, index=None):
        if index is None:
            if not spare:
                spare.append(used[0])
                used[0] += 1
            index = spare.pop(0)
        assert used[0] <= sends

        def make():
            return copy(src, dst, ssem.at[index], recv_sem, device)

        run_if(condition, lambda: make().start())
        pending.append((condition, lambda: make().wait_send(), index))
        return index

    def reserve(size):
        base = used[0]
        used[0] += size
        return base

    def by_distance(d, act):
        for there, toward in ((o - d, 1), (o + d, -1)):
            valid = (there >= 0) & (there < outer_n)
            act(jnp.clip(there, 0, outer_n - 1), valid, toward)

    def drain(first):
        for condition, finish_send, index in pending[:first]:
            run_if(condition, finish_send)
            if isinstance(index, int) and index not in spare:
                spare.append(index)
        del pending[:first]

    def arrive(dst, recv_sem, condition=None):
        run_if(
            condition,
            lambda: copy(dst, dst, ssem.at[0], recv_sem, dev(o, i, x, other)).wait_recv(),
        )

    partner = dev(o, i, x, other)
    beside = dev(o, i, 1 - x, k)

    right, left = o + 1 < outer_n, o > 0
    halves = [slice(c * chunk, (c + 1) * chunk) for c in range(2)]
    fetches[0].wait()
    for c, at in enumerate(halves):
        for step, condition in ((1, right), (-1, left)):
            launch(
                tok_in.at[t, :, at],
                stage.at[c, o],
                r_tok.at[c, o],
                dev(o + step, i, x, k),
                condition,
            )

    is_q, is_l = x == 0, x != 0
    extra_o, extra_unit = 1 + x, outer_n + x
    extra = o == extra_o
    for fetch in fetches[6:8]:
        fetch.wait()
    for d in range(1, outer_n):
        there, index = turn_o(d), None
        for source, condition in ((q_down, is_q), (l_down, is_l)):
            index = launch(
                source.at[k, :, lane(there)],
                l_all.at[0, i, o, k],
                r_lat_w.at[0, i, o],
                dev(there, i, x, k),
                condition,
                index,
            )
    launch(
        q_down.at[k, :, lane(extra_unit)],
        l_all.at[1, i, o, k],
        r_lat_w.at[1, i, o],
        dev(extra_o, i, x, k),
        jnp.logical_not(extra),
    )
    for fetch in fetches[1:6] + fetches[8:]:
        fetch.wait()

    def send_weights(g):
        first, count = groups[g]
        for m in range(first, first + count):
            for h in range(heads):
                there = heads * k + h
                for r in range(2):
                    launch(
                        mats[m].at[r, :, h * LANES : (h + 1) * LANES],
                        w_all.at[i, o, m, r],
                        r_rec_w.at[g, i, o],
                        dev(there, i, x, r),
                        there != o,
                    )

    def send_home_weights(g):
        first, count = groups[g]
        for m in range(first, first + count):
            launch(
                mats[m].at[other, :, lane(hh)],
                w_all.at[i, o, m, other],
                r_rec_w.at[g, i, o],
                partner,
                at_home,
            )

    def out_piece(j, i_, o_):
        return out_w.at[j, i_, o_], r_out.at[j, i_, o_]

    outs = (chain_out, attend_out)
    send_home_weights(0)
    for j, (source, target) in enumerate(
        (
            (query_up, up_q),
            (latent_up.at[:, lane(hh, 2 * LANES)], up_l),
            (rate_in, rate_ref),
            (chain_gain_in, chain_gain_ref),
            (mixer_gain_in, mixer_gain_ref),
        )
    ):
        launch(source, target, r_small.at[j], partner, at_home)
    send_home_weights(1)

    @pl.when(is_q)
    def _():
        l_all[0, i, o, k] = q_down[k, :, lane(o)]

    @pl.when(is_l)
    def _():
        l_all[0, i, o, k] = l_down[k, :, lane(o)]

    @pl.when(extra)
    def _():
        l_all[1, i, o, k] = q_down[k, :, lane(extra_unit)]

    @pl.when(at_home)
    def _():
        for m in range(len(mats)):
            w_all[i, o, m, k] = mats[m][k, :, lane(hh)]
        up_q[...] = query_up[...]
        up_l[...] = latent_up[:, lane(hh, 2 * LANES)]
        rate_ref[...] = rate_in[...]
        chain_gain_ref[...] = chain_gain_in[...]
        mixer_gain_ref[...] = mixer_gain_in[...]

    def lat_piece(slot, i_, o_):
        return l_all.at[slot, i_, o_, k], r_lat_w.at[slot, i_, o_]

    def lat_block(slot, i_, half):
        return l_all.at[slot, i_, :, half], r_lat_p.at[slot, i_]

    def rec_piece(g, i_, o_):
        first, count = groups[g]
        return w_all.at[i_, o_, first : first + count, k], r_rec_w.at[g, i_, o_]

    def rec_block(g, i_, half):
        first, count = groups[g]
        return w_all.at[i_, :, first : first + count, half], r_rec_p.at[g, i_]

    def own_line(piece, condition=None, own=None):
        ref, sem = piece[0](i, o)
        if own is not None:
            arrive(ref, sem, own)
        for e in range(1, inner_n):
            launch(ref, ref, sem, dev(o, turn_i(e), x, k), condition)

    def from_line(piece, d, condition=None):
        def act(there, valid, toward):
            valid = both(valid, condition)
            ref, sem = piece[0](i, there)
            arrive(ref, sem, valid)
            for e in range(1, inner_n):
                launch(ref, ref, sem, dev(o, turn_i(e), x, k), valid, piece[2][e] + there)

        by_distance(d, act)
        if d == outer_n - 1:
            launch(*pair(piece[1], i, k), partner, condition)

    def pair(block, i_, half):
        ref, sem = block(i_, half)
        return ref, ref, sem

    def from_pairs(piece, condition=None):
        for e in range(1, inner_n):
            for d in range(outer_n):
                arrive(*piece[0](turn_i(e), turn_o(d)), condition)
            launch(*pair(piece[1], turn_i(e), k), partner, condition)

    def from_partner(piece, condition=None):
        for e in range(inner_n):
            arrive(*piece[1](turn_i(e), other), condition)

    def kind(piece, block, which):
        marks = [reserve(outer_n) for _ in range(inner_n)]
        return functools.partial(piece, which), functools.partial(block, which), marks

    lat_a, lat_b = kind(lat_piece, lat_block, 0), kind(lat_piece, lat_block, 1)
    rec = [kind(rec_piece, rec_block, g) for g in range(2)]
    own_line(lat_a)
    own_line(lat_b, extra)

    for b in range(blocks):

        @pl.when(blocks * k + b == o)
        def _():
            tok[b] = tok_in[...]

    sign_pick = spread(ATT_QK, 0, True)[NOPE_DIM:, LANES:].astype(bf16)
    depth = width // n
    rot_all[...] = (
        lax.dot_general(
            rot_down[...], sign_pick, (((0,), (0,)), ((), ())), preferred_element_type=f32
        )
        .astype(bf16)
        .reshape(n, depth, 2 * LANES)
    )

    own_line(rec[0], None, away)
    for j in range(2):
        for e in range(1, inner_n):
            launch(outs[j], *out_piece(j, i, o), dev(o, turn_i(e), x, k))
    own_line(rec[1], None, away)

    def gains(ref):
        wide = jnp.broadcast_to(ref[...], (8, ATT_QK))
        return jnp.dot(
            wide,
            spread(ATT_QK, 0, False),
            precision=lax.Precision.HIGHEST,
            preferred_element_type=f32,
        )[0:1]

    for j, target in enumerate((up_q, up_l, rate_ref, chain_gain_ref, mixer_gain_ref)):
        arrive(target, r_small.at[j], away)
    up_q[...] = jnp.dot(
        up_q[...],
        spread(heads * ATT_QK, hh * ATT_QK, True).astype(bf16),
        preferred_element_type=f32,
    ).astype(bf16)

    marks = [[reserve(outer_n) for _ in range(3)] for _ in range(2)]

    def relay_tokens(c, there, valid, toward, last):
        ref, sem = stage.at[c, there], r_tok.at[c, there]
        arrive(ref, sem, valid)
        if not last:
            onward = both(valid, right if toward > 0 else left)
            launch(ref, ref, sem, dev(o + toward, i, x, k), onward, marks[c][0] + there)
        core, b = there // blocks, lax.rem(there, blocks)
        at = halves[c]
        target, sem = tok.at[b, t, :, at], r_deliver.at[c, b, t]
        launch(ref, target, sem, dev(o, i, 1 - x, core), valid, marks[c][1] + there)
        launch(ref, target, sem, partner, both(valid, core != k), marks[c][2] + there)

        @pl.when(both(valid, core == k))
        def _():
            tok[b, t, :, at] = stage[c, there]

    for d in range(1, outer_n):
        for c in range(2):
            by_distance(
                d,
                functools.partial(
                    lambda c, there, valid, toward: relay_tokens(
                        c, there, valid, toward, d == outer_n - 1
                    ),
                    c,
                ),
            )
        if d == 1:
            from_line(lat_a, 1)
            from_line(lat_b, 1, extra)
        if d == outer_n - 2:
            send_weights(0)
            for far_d in range(2, outer_n):
                from_line(lat_a, far_d)
                from_line(lat_b, far_d, extra)

    from_pairs(lat_a)
    from_pairs(lat_b, extra)

    for b in range(blocks):
        there = blocks * k + b
        for d in range(1, heads_n):
            q = lax.rem(t + d, heads_n)
            for c, at in enumerate(halves):
                arrive(tok.at[b, q, :, at], r_deliver.at[c, b, q], there != o)
        wide = jnp.concatenate([tok[b, q].astype(f32) for q in range(heads_n)], axis=0)
        scale = inverse_rms(wide, width)
        normed = (wide * scale * input_gain[...]).astype(bf16)
        for s in range(n):
            xs[s, b * rows : (b + 1) * rows, :] = normed[:, s * depth : (s + 1) * depth]

    def project(rhs, columns):
        def body(s, total):
            return total + jnp.dot(xs[s], rhs(s), preferred_element_type=f32)

        return lax.fori_loop(
            0, n, body, jnp.zeros((blocks * rows, columns), f32), unroll=n <= 8
        ).astype(bf16)

    from_partner(lat_a)
    from_partner(lat_b, extra)
    own_unit = x * q_units + o
    first = project(
        lambda s: jnp.concatenate([l_all[0, lax.rem(s, inner_n), s // inner_n].reshape(depth, LANES), rot_all[s]], axis=1),
        3 * LANES,
    )
    lat[own_unit] = first[:, :LANES]
    rotary = first[:, LANES:].astype(f32)

    @pl.when(extra)
    def _():
        lat[extra_unit] = project(lambda s: l_all[1, lax.rem(s, inner_n), s // inner_n].reshape(depth, LANES), LANES)

    def send_unit(unit, condition=None):
        for d in range(1, outer_n):
            launch(lat.at[unit], lat.at[unit], r_lat.at[unit], dev(turn_o(d), i, x, k), condition)
        launch(lat.at[unit], lat.at[unit], r_lat.at[unit], beside, condition)

    early = len(pending)
    send_unit(own_unit)
    send_unit(extra_unit, extra)
    for d in range(1, outer_n):
        from_line(rec[0], d)

    marks_x = reserve(outer_n)

    def relay_unit(there, valid, toward):
        unit = x * q_units + there
        arrive(lat.at[unit], r_lat.at[unit], valid)
        launch(lat.at[unit], lat.at[unit], r_lat.at[unit], beside, valid, marks_x + there)

    for d in range(1, outer_n):
        by_distance(d, relay_unit)
    arrive(lat.at[extra_unit], r_lat.at[extra_unit], jnp.logical_not(extra))
    launch(
        lat.at[extra_unit],
        lat.at[extra_unit],
        r_lat.at[extra_unit],
        beside,
        jnp.logical_not(extra),
    )
    send_weights(1)

    marks_out = [[reserve(outer_n) for _ in range(inner_n)] for _ in range(2)]
    for j in range(2):
        ref, sem = out_piece(j, i, o)
        for step, condition in ((1, right), (-1, left)):
            launch(outs[j], ref, sem, dev(o + step, i, x, k), condition)
        out_w[j, i, o] = outs[j][...]

    def relay_out(d):
        for j in range(2):

            def act(there, valid, toward):
                ref, sem = out_piece(j, i, there)
                arrive(ref, sem, valid)
                if d < outer_n - 1:
                    onward = both(valid, right if toward > 0 else left)
                    launch(ref, ref, sem, dev(o + toward, i, x, k), onward, marks_out[j][0] + there)
                for e in range(1, inner_n):
                    launch(
                        ref, ref, sem, dev(o, turn_i(e), x, k), valid, marks_out[j][e] + there
                    )

            by_distance(d, act)

    from_pairs(rec[0])

    def shared(ref, sem):
        for e in range(1, inner_n):
            launch(ref, ref, sem, dev(o, turn_i(e), x, k))
        launch(ref, ref, sem, partner)

    def columns(s, mats_here):
        return jnp.concatenate([
                w_all[lax.rem(s, inner_n), s // inner_n, m].reshape(depth, LANES)
                for m in mats_here
            ], axis=1)

    from_partner(rec[0])
    vfb = project(lambda s: columns(s, (0, 1, 2)), 3 * LANES)
    value = [vfb[b * rows : (b + 1) * rows, :LANES] for b in range(blocks)]
    row = lax.broadcasted_iota(jnp.int32, (rows, rows), 0)
    col = lax.broadcasted_iota(jnp.int32, (rows, rows), 1)
    masks = (row >= col, row <= col)

    def direction(d):
        rate = rate_ref[d : d + 1, lane(hh)] / (rows * n)
        logit = vfb[:, (1 + d) * LANES : (2 + d) * LANES].astype(f32)
        key = rate * jax.nn.sigmoid(-logit)
        decay = jnp.log1p(-key)
        total = jnp.dot(
            jnp.where(masks[d], 1.0, 0.0),
            jnp.concatenate([decay[b * rows : (b + 1) * rows] for b in range(blocks)], axis=1),
            precision=lax.Precision.HIGHEST,
            preferred_element_type=f32,
        )
        keys, totals = [], []
        last = (rows - 1, 0)[d]
        for b in range(blocks):
            part = total[:, b * LANES : (b + 1) * LANES]
            full = part[last : last + 1, :]
            near = (key[b * rows : (b + 1) * rows] * jnp.exp(-part)).astype(bf16)
            state = lax.dot_general(
                value[b], near, (((0,), (0,)), ((), ())), preferred_element_type=f32
            )
            states[i, blocks * k + b, d] = (state * jnp.exp(full)).astype(bf16)
            logs[i, blocks * k + b, d] = jnp.broadcast_to(full, (8, LANES))
            keys.append(near)
            totals.append(part)
        return keys, totals

    near = [direction(d) for d in range(2)]

    def state_pieces(i_, k_):
        at = pl.ds(k_ * blocks, blocks)
        return (states.at[i_, at], r_state.at[i_, k_]), (logs.at[i_, at], r_log.at[i_, k_])

    for ref, sem in state_pieces(i, k):
        shared(ref, sem)

    drain(early)
    for d in range(outer_n):
        unit = (1 - x) * q_units + turn_o(d)
        arrive(lat.at[unit], r_lat.at[unit])
    far_unit = outer_n + 1 - x
    arrive(lat.at[far_unit], r_lat.at[far_unit])

    cosines, sines = [], []
    for b in range(blocks):
        s = (blocks * k + b) * inner_n + i
        cb, sb = cos_block[pl.ds(s, 1), :], sin_block[pl.ds(s, 1), :]
        cosines.append(cb * cos_row[...] - sb * sin_row[...])
        sines.append(sb * cos_row[...] + cb * sin_row[...])
    cosine = jnp.concatenate(cosines, axis=0)
    sine = jnp.concatenate(sines, axis=0)

    def latent(first_unit, count, gain):
        wide = jnp.concatenate(
            [lat[u].astype(f32) for u in range(first_unit, first_unit + count)], axis=1
        )
        scaling = jnp.concatenate([gain[u : u + 1] for u in range(count)], axis=1)
        return (wide * inverse_rms(wide, count * LANES) * scaling).astype(bf16)

    def finish(plain, tail, swapped, gain):
        square = jnp.sum(plain * plain + tail * tail, axis=-1, keepdims=True)
        scale = lax.rsqrt(square / ATT_QK + norm_eps)
        turned = tail * gain[:, LANES : 2 * LANES] * cosine + swapped * gain[:, 2 * LANES :] * sine
        return jnp.concatenate(
            [(plain * scale * gain[:, :LANES]).astype(bf16), (turned * scale).astype(bf16)], axis=1
        )

    pairs = jnp.dot(
        latent(q_units, outer_n, latent_gain), up_l[...], preferred_element_type=f32
    ).astype(bf16)
    kv[i, k, :, : 2 * LANES] = finish(
        pairs[:, :LANES].astype(f32), rotary[:, :LANES], rotary[:, LANES:], gains(key_gain)
    )
    kv[i, k, :, 2 * LANES :] = pairs[:, LANES:]

    shared(kv.at[i, k], r_kv.at[i, k])

    attend_q = (
        jnp.dot(latent(0, q_units, query_latent_gain), up_q[...], preferred_element_type=f32)
        .astype(bf16)
        .astype(f32)
    )
    query = finish(
        attend_q[:, :LANES],
        attend_q[:, LANES : 2 * LANES],
        attend_q[:, 2 * LANES :],
        gains(query_gain),
    )


    scale = ATT_QK ** (-0.5) * 1.4426950408889634

    def attend(carry, i_, k_):
        numer, denom = carry
        score = against(query, kv[i_, k_, :, : 2 * LANES])
        weight = jnp.exp2(score * scale)
        numer += jnp.dot(
            weight.astype(bf16), kv[i_, k_, :, 2 * LANES :], preferred_element_type=f32
        )
        return numer, denom + jnp.sum(weight, axis=-1, keepdims=True)

    carry = (jnp.zeros((blocks * rows, LANES), f32), jnp.zeros((blocks * rows, 1), f32))
    relay_out(1)
    carry = attend(carry, i, k)
    arrive(kv.at[i, other], r_kv.at[i, other])
    carry = attend(carry, i, other)
    for d in range(1, outer_n):
        from_line(rec[1], d)

    def relay_pair(ref, sem):
        arrive(ref, sem)
        launch(ref, ref, sem, partner)

    for e in range(1, inner_n):
        relay_pair(kv.at[turn_i(e), k], r_kv.at[turn_i(e), k])
    relay_out(2)
    for e in range(1, inner_n):
        for ref, sem in state_pieces(turn_i(e), k):
            relay_pair(ref, sem)
    from_pairs(rec[1])
    for e in range(1, inner_n):
        there = turn_i(e)
        carry = attend(carry, there, k)
        arrive(kv.at[there, other], r_kv.at[there, other])
        carry = attend(carry, there, other)
    rows_out = carry[0] / carry[1]
    attend_mixed = (
        rows_out * inverse_rms(rows_out, LANES) * mixer_gain_ref[:, lane(hh)]
    ).astype(bf16)

    for d in range(3, outer_n):
        relay_out(d)

    from_partner(rec[1])
    qg = project(lambda s: columns(s, (3, 4)), 2 * LANES).astype(f32)
    for e in range(inner_n):
        for k_ in (k, other):
            if e or k_ is other:
                for ref, sem in state_pieces(turn_i(e), k_):
                    if k_ is other:
                        arrive(ref, sem)

    def forward(s, state):
        i_, o_ = lax.rem(s, inner_n), s // inner_n
        return state * jnp.exp(logs[i_, o_, 0, 0:1, :]) + states[i_, o_, 0].astype(f32)

    def backward(j, state):
        s = n - 1 - j
        i_, o_ = lax.rem(s, inner_n), s // inner_n
        return state * jnp.exp(logs[i_, o_, 1, 0:1, :]) + states[i_, o_, 1].astype(f32)

    nothing = jnp.zeros((LANES, LANES), f32)
    for b in range(blocks):
        there = blocks * k + b
        s = there * inner_n + i
        incoming = (
            lax.fori_loop(0, s, forward, nothing).astype(bf16),
            lax.fori_loop(0, n - 1 - s, backward, nothing).astype(bf16),
        )
        at = slice(b * rows, (b + 1) * rows)
        total = jnp.zeros((rows, LANES), f32)
        within = jnp.zeros((rows, rows), f32)
        for d in range(2):
            keys, totals = near[d]
            probe = (qg[at, :LANES] * jnp.exp(totals[b])).astype(bf16)
            within += jnp.where(masks[d], against(probe, keys[b]), 0.0)
            total += against(probe, incoming[d])
        total += jnp.dot(within.astype(bf16), value[b], preferred_element_type=f32)
        gate = qg[at, LANES:]
        scaled = total * inverse_rms(total, LANES) * chain_gain_ref[:, lane(hh)]
        mix_send[b, :, :LANES] = (scaled * (gate * jax.nn.sigmoid(gate))).astype(bf16)
        mix_send[b, :, LANES:] = attend_mixed[at]
        home = there == o
        launch(
            mix_send.at[b],
            mix_recv.at[hh],
            r_mix.at[hh],
            dev(there, i, x, o // heads),
            jnp.logical_not(home),
        )

        @pl.when(home)
        def _():
            mix_recv[hh] = mix_send[b]

    for j in range(2):
        for e in range(1, inner_n):
            for d in range(outer_n):
                arrive(*out_piece(j, turn_i(e), turn_o(d)))
    for h in range(heads):
        arrive(mix_recv.at[h], r_mix.at[h], heads * k + h != o)
    col_n = out_w.shape[4]
    spans = [range(c * n // 2, (c + 1) * n // 2) for c in range(2)]
    own_rows = 2 * part_rows

    def partial(c, x_):
        at = pl.ds(pl.multiple_of(x_ * own_rows, own_rows), own_rows)
        chain_part = jnp.concatenate([mix_recv[h, at, :LANES] for h in range(heads)], axis=1)
        attend_part = jnp.concatenate([mix_recv[h, at, LANES:] for h in range(heads)], axis=1)
        return [
            jnp.dot(chain_part, out_w[0, s % inner_n, s // inner_n], preferred_element_type=f32)
            + jnp.dot(attend_part, out_w[1, s % inner_n, s // inner_n], preferred_element_type=f32)
            for s in spans[c]
        ]

    def spread_rows(target, c, x_):
        for j, product in enumerate(partial(c, x_)):
            at = slice(j * col_n, (j + 1) * col_n)
            for q in range(2):
                target[c, q, :, at] = product[q * part_rows : (q + 1) * part_rows]

    for c in range(2):
        spread_rows(part_far, c, 1 - x)
        send_far[c] = part_far[c, other].astype(bf16)
        launch(send_far.at[c], got_far.at[c], r_sum.at[0, c], partner)
    for c in range(2):
        arrive(got_far.at[c], r_sum.at[0, c])
        send_x[c] = (part_far[c, k] + got_far[c].astype(f32)).astype(bf16)
        launch(send_x.at[c], got_x.at[c], r_sum.at[1, c], beside)
    for c in range(2):
        spread_rows(part_near, c, x)
        send_near[c] = part_near[c, other].astype(bf16)
        launch(send_near.at[c], got_near.at[c], r_sum.at[2, c], partner)
    for c in range(2):
        arrive(got_near.at[c], r_sum.at[2, c])
        arrive(got_x.at[c], r_sum.at[1, c])
        size = len(spans[c]) * col_n
        out_ref[:, c * size : (c + 1) * size] = (
            part_near[c, k] + got_near[c].astype(f32) + got_x[c].astype(f32)
        )
    drain(len(pending))
    needed.append(used[0])


def on_device(
    tokens,
    input_gain,
    chain_query,
    forward_gate,
    backward_gate,
    chain_value,
    output_gate,
    forget_rate,
    chain_gain,
    query_down,
    latent_down,
    rotary_down,
    query_latent_gain,
    latent_gain,
    query_up,
    latent_up,
    query_head_gain,
    key_head_gain,
    mixer_gain,
    chain_out,
    attend_out,
):
    n, heads_n = lax.axis_size("sp"), lax.axis_size("tp")
    rows, width = tokens.shape
    depth = chain_query.shape[0]
    heads = query_up.shape[1] // ATT_QK
    outer_n = 2 * heads
    inner_n = n // outer_n
    blocks = outer_n // 2
    half = depth // 2
    units = (query_down.shape[1] + latent_down.shape[1]) // LANES
    part = rows // heads_n
    out_cols = n * chain_out.shape[1]

    inverse = rope_theta ** (-np.arange(0, ROPE_DIM, 2) / ROPE_DIM)

    def table(positions):
        angles = np.tile(positions[:, None] * inverse, (1, 2))
        pad = ((0, 0), (0, LANES - ROPE_DIM))
        return [jnp.asarray(np.pad(f(angles), pad), f32) for f in (np.cos, np.sin)]

    in_row = table(np.arange(rows, dtype=np.float64))
    in_block = table(np.arange(n, dtype=np.float64) * rows)

    def halves(w):
        return w.reshape(2, half, w.shape[1])

    operands = (
        tokens.reshape(heads_n, part, width),
        *[
            halves(w)
            for w in (
                chain_value,
                forward_gate,
                backward_gate,
                chain_query,
                output_gate,
                query_down,
                latent_down,
            )
        ],
        rotary_down.T,
        query_up,
        latent_up,
        chain_out,
        attend_out,
        forget_rate,
        chain_gain[None],
        mixer_gain[None],
        input_gain[None],
        query_latent_gain.reshape(-1, LANES),
        latent_gain.reshape(-1, LANES),
        query_head_gain[None],
        key_head_gain[None],
        *in_row,
        *in_block,
    )
    dma = pltpu.SemaphoreType.DMA
    vmem = pl.BlockSpec(memory_space=pltpu.VMEM)
    tall = blocks * rows
    needed = []
    hbm = pl.BlockSpec(memory_space=pltpu.HBM)
    big = operands[:13]

    def build(sends):
      return pl.pallas_call(
        functools.partial(mixer_kernel, n, heads_n, heads, sends, needed),
        out_shape=jax.ShapeDtypeStruct((part, out_cols), f32),
        in_specs=[hbm] * len(big) + [vmem] * (len(operands) - len(big)),
        out_specs=vmem,
        scratch_shapes=[
            pltpu.VMEM((2, outer_n, part, width // 2), bf16),
            pltpu.VMEM((blocks, heads_n, part, width), bf16),
            pltpu.VMEM((n, tall, depth), bf16),
            pltpu.VMEM((inner_n, outer_n, 5, 2, half, LANES), bf16),
            pltpu.VMEM((2, inner_n, outer_n, 2, half, LANES), bf16),
            pltpu.VMEM((n, depth, 2 * LANES), bf16),
            pltpu.VMEM((units, tall, LANES), bf16),
            pltpu.VMEM(forget_rate.shape, f32),
            pltpu.VMEM((1,) + chain_gain.shape, f32),
            pltpu.VMEM((1,) + mixer_gain.shape, f32),
            pltpu.VMEM(query_up.shape, bf16),
            pltpu.VMEM((latent_up.shape[0], 2 * LANES), bf16),
            pltpu.VMEM((inner_n, 2, tall, 3 * LANES), bf16),
            pltpu.VMEM((inner_n, outer_n, 2, LANES, LANES), bf16),
            pltpu.VMEM((inner_n, outer_n, 2, 8, LANES), f32),
            pltpu.VMEM((blocks, rows, 2 * LANES), bf16),
            pltpu.VMEM((heads, rows, 2 * LANES), bf16),
            pltpu.VMEM((2, inner_n, outer_n) + chain_out.shape, bf16),
            pltpu.VMEM((2, 2, part, out_cols // 2), f32),
            pltpu.VMEM((2, 2, part, out_cols // 2), f32),
            pltpu.VMEM((2, part, out_cols // 2), bf16),
            pltpu.VMEM((2, part, out_cols // 2), bf16),
            pltpu.VMEM((2, part, out_cols // 2), bf16),
            pltpu.VMEM((2, part, out_cols // 2), bf16),
            pltpu.VMEM((2, part, out_cols // 2), bf16),
            pltpu.VMEM((2, part, out_cols // 2), bf16),
            dma((sends,)),
            dma((2, outer_n)),
            dma((2, blocks, heads_n)),
            dma((2, inner_n, outer_n)),
            dma((2, inner_n)),
            dma((2, inner_n, outer_n)),
            dma((2, inner_n)),
            dma((5,)),
            dma((units,)),
            dma((inner_n, 2)),
            dma((inner_n, 2)),
            dma((inner_n, 2)),
            dma((heads,)),
            dma((2, inner_n, outer_n)),
            dma((3, 2)),
        ]
        + [pltpu.VMEM(a.shape, a.dtype) for a in big]
        + [dma((len(big),))],
        compiler_params=pltpu.CompilerParams(
            collective_id=0, has_side_effects=True, vmem_limit_bytes=VMEM_LIMIT
        ),
      )

    jax.eval_shape(build(200 + 30 * n), *operands)
    return build(needed[0])(*operands)


def solution(mesh):
    placed = (
        P("sp", None),
        P(),
        P("sp", "tp"),
        P("sp", "tp"),
        P("sp", "tp"),
        P("sp", "tp"),
        P("sp", "tp"),
        P(None, "tp"),
        P("tp"),
        P("sp", None),
        P("sp", None),
        P(),
        P(),
        P(),
        P(None, "tp"),
        P(None, "tp"),
        P(),
        P(),
        P("tp"),
        P("tp", "sp"),
        P("tp", "sp"),
    )
    return jax.shard_map(
        on_device, mesh=mesh, in_specs=placed, out_specs=P(("sp", "tp"), None), check_vma=False
    )
```

```python
import functools

import jax
import jax.numpy as jnp
import numpy as np
from jax import lax
from jax.experimental import pallas as pl
from jax.experimental.pallas import tpu as pltpu
from jax.sharding import PartitionSpec as P

LANES = 128
RING = 64
NOPE_DIM = 128
ROPE_DIM = 64
ATT_QK = 192
HALF = ROPE_DIM // 2

norm_eps = 1e-06
rope_theta = 10000.0
MESH = pl.DeviceIdType.MESH
VMEM_LIMIT = 48 * 1024 * 1024
f32 = jnp.float32
bf16 = jnp.bfloat16


def run_if(condition, act):
    if condition is None:
        act()
    else:
        pl.when(condition)(act)


def both(a, b):
    if a is None:
        return b
    if b is None:
        return a
    return jnp.logical_and(a, b)


def against(a, b):
    return lax.dot_general(a, b, (((1,), (1,)), ((), ())), preferred_element_type=f32)


def inverse_rms(values, size):
    return lax.rsqrt(jnp.sum(values * values, axis=-1, keepdims=True) / size + norm_eps)


def spread(count, start, signed):
    row = lax.broadcasted_iota(jnp.int32, (count, 3 * LANES), 0) - start
    col = lax.broadcasted_iota(jnp.int32, (count, 3 * LANES), 1)
    straight = (col < ATT_QK) & (row == col)
    at = col - 2 * LANES
    low = (at >= 0) & (at < HALF) & (row == NOPE_DIM + HALF + at)
    high = (at >= HALF) & (at < ROPE_DIM) & (row == NOPE_DIM + at - HALF)
    return (
        jnp.where(straight, 1.0, 0.0)
        + jnp.where(low, -1.0 if signed else 1.0, 0.0)
        + jnp.where(high, 1.0, 0.0)
    )


def mixer_kernel(n, heads_n, heads, sends, needed, *refs):
    count = 13
    far, near_by = refs[:count], refs[-count - 1 : -1]
    fetched = refs[-1]
    (
        tok_in,
        wv,
        wf,
        wb,
        wq,
        wg,
        q_down,
        l_down,
        rot_down,
        query_up,
        latent_up,
        chain_out,
        attend_out,
    ) = near_by
    (
        rate_in,
        chain_gain_in,
        mixer_gain_in,
        input_gain,
        query_latent_gain,
        latent_gain,
        query_gain,
        key_gain,
        cos_row,
        sin_row,
        cos_block,
        sin_block,
        out_ref,
        stage,
        tok,
        xs,
        w_all,
        l_all,
        rot_all,
        lat,
        rate_ref,
        chain_gain_ref,
        mixer_gain_ref,
        up_q,
        up_l,
        kv,
        states,
        logs,
        mix_send,
        mix_recv,
        out_w,
        part_far,
        part_near,
        send_far,
        send_near,
        got_far,
        got_near,
        send_x,
        got_x,
        ssem,
        r_tok,
        r_deliver,
        r_lat_w,
        r_lat_p,
        r_rec_w,
        r_rec_p,
        r_small,
        r_lat,
        r_kv,
        r_state,
        r_log,
        r_mix,
        r_out,
        r_sum,
    ) = refs[count : -count - 1]
    mats = (wv, wf, wb, wq, wg)
    groups = ((0, 3), (3, 2))
    outer_n = 2 * heads
    inner_n = n // outer_n
    blocks = outer_n // 2
    part_rows, width = tok_in.shape[1:]
    chunk = width // 2
    rows = part_rows * heads_n
    q_units = q_down.shape[2] // LANES

    me = lax.axis_index("sp")
    t = lax.axis_index("tp")
    o, i = me // inner_n, lax.rem(me, inner_n)
    x, k = t // 2, lax.rem(t, 2)
    other = 1 - k
    at_home = (o // heads) == k
    away = jnp.logical_not(at_home)
    hh = lax.rem(o, heads)

    def dev(o_, i_, x_, k_):
        return {"sp": o_ * inner_n + i_, "tp": x_ * 2 + k_}

    def turn_o(d):
        return lax.rem(o + d, outer_n)

    def turn_i(d):
        return lax.rem(i + d, inner_n)

    def lane(index, size=LANES):
        return pl.ds(pl.multiple_of(index * size, LANES), size)

    peers = [dev(turn_o(d), i, x, r) for d in range(1, outer_n) for r in range(2)]
    peers += [dev(o, turn_i(d), x, k) for d in range(1, inner_n)]
    peers += [{"sp": me, "tp": lax.rem(t + d, heads_n)} for d in range(1, heads_n)]
    fetches = [pltpu.make_async_copy(far[j], near_by[j], fetched.at[j]) for j in range(count)]
    for fetch in fetches:
        fetch.start()
    barrier = pltpu.get_barrier_semaphore()
    for peer in peers:
        pl.semaphore_signal(barrier, inc=1, device_id=peer, device_id_type=MESH)
    pl.semaphore_wait(barrier, len(peers))

    pending, used, shared_slots = [], [0], set()
    ring = min(sends, RING)

    def copy(src, dst, send_sem, recv_sem, device):
        return pltpu.make_async_remote_copy(
            src_ref=src,
            dst_ref=dst,
            send_sem=send_sem,
            recv_sem=recv_sem,
            device_id=device,
            device_id_type=MESH,
        )

    def launch(src, dst, recv_sem, device, condition=None, index=None):
        if index is None:
            if used[0] < ring:
                index = used[0]
                used[0] += 1
            else:
                at = next(a for a, entry in enumerate(pending) if entry[2] not in shared_slots)
                finished, finish_send, index = pending.pop(at)
                run_if(finished, finish_send)

        def make():
            return copy(src, dst, ssem.at[index], recv_sem, device)

        run_if(condition, lambda: make().start())
        pending.append((condition, lambda: make().wait_send(), index))
        return index

    def by_distance(d, act):
        for there, toward in ((o - d, 1), (o + d, -1)):
            valid = (there >= 0) & (there < outer_n)
            act(jnp.clip(there, 0, outer_n - 1), valid, toward)

    def drain():
        for condition, finish_send, _ in pending:
            run_if(condition, finish_send)

    def arrive(dst, recv_sem, condition=None):
        run_if(
            condition,
            lambda: copy(dst, dst, ssem.at[0], recv_sem, dev(o, i, x, other)).wait_recv(),
        )

    partner = dev(o, i, x, other)
    beside = dev(o, i, 1 - x, k)

    right, left = o + 1 < outer_n, o > 0
    halves = [slice(c * chunk, (c + 1) * chunk) for c in range(2)]
    fetches[0].wait()
    for c, at in enumerate(halves):
        for step, condition in ((1, right), (-1, left)):
            launch(
                tok_in.at[t, :, at],
                stage.at[c, o],
                r_tok.at[c, o],
                dev(o + step, i, x, k),
                condition,
            )

    is_q, is_l = x == 0, x != 0
    extra_o, extra_unit = 1 + x, outer_n + x
    extra = o == extra_o
    for fetch in fetches[6:8]:
        fetch.wait()
    for d in range(1, outer_n):
        there, index = turn_o(d), None
        for source, condition in ((q_down, is_q), (l_down, is_l)):
            index = launch(
                source.at[k, :, lane(there)],
                l_all.at[0, i, o, k],
                r_lat_w.at[0, i, o],
                dev(there, i, x, k),
                condition,
                index,
            )
        shared_slots.add(index)
    launch(
        q_down.at[k, :, lane(extra_unit)],
        l_all.at[1, i, o, k],
        r_lat_w.at[1, i, o],
        dev(extra_o, i, x, k),
        jnp.logical_not(extra),
    )
    for fetch in fetches[1:6] + fetches[8:]:
        fetch.wait()

    def send_weights(g):
        first, count = groups[g]
        for m in range(first, first + count):
            for h in range(heads):
                there = heads * k + h
                for r in range(2):
                    launch(
                        mats[m].at[r, :, h * LANES : (h + 1) * LANES],
                        w_all.at[i, o, m, r],
                        r_rec_w.at[g, i, o],
                        dev(there, i, x, r),
                        there != o,
                    )

    def send_home_weights(g):
        first, count = groups[g]
        for m in range(first, first + count):
            launch(
                mats[m].at[other, :, lane(hh)],
                w_all.at[i, o, m, other],
                r_rec_w.at[g, i, o],
                partner,
                at_home,
            )

    def out_piece(j, i_, o_):
        return out_w.at[j, i_, o_], r_out.at[j, i_, o_]

    outs = (chain_out, attend_out)
    send_home_weights(0)
    for j, (source, target) in enumerate(
        (
            (query_up, up_q),
            (latent_up.at[:, lane(hh, 2 * LANES)], up_l),
            (rate_in, rate_ref),
            (chain_gain_in, chain_gain_ref),
            (mixer_gain_in, mixer_gain_ref),
        )
    ):
        launch(source, target, r_small.at[j], partner, at_home)
    send_home_weights(1)

    @pl.when(is_q)
    def _():
        l_all[0, i, o, k] = q_down[k, :, lane(o)]

    @pl.when(is_l)
    def _():
        l_all[0, i, o, k] = l_down[k, :, lane(o)]

    @pl.when(extra)
    def _():
        l_all[1, i, o, k] = q_down[k, :, lane(extra_unit)]

    @pl.when(at_home)
    def _():
        for m in range(len(mats)):
            w_all[i, o, m, k] = mats[m][k, :, lane(hh)]
        up_q[...] = query_up[...]
        up_l[...] = latent_up[:, lane(hh, 2 * LANES)]
        rate_ref[...] = rate_in[...]
        chain_gain_ref[...] = chain_gain_in[...]
        mixer_gain_ref[...] = mixer_gain_in[...]

    def lat_piece(slot, i_, o_):
        return l_all.at[slot, i_, o_, k], r_lat_w.at[slot, i_, o_]

    def lat_block(slot, i_, half):
        return l_all.at[slot, i_, :, half], r_lat_p.at[slot, i_]

    def rec_piece(g, i_, o_):
        first, count = groups[g]
        return w_all.at[i_, o_, first : first + count, k], r_rec_w.at[g, i_, o_]

    def rec_block(g, i_, half):
        first, count = groups[g]
        return w_all.at[i_, :, first : first + count, half], r_rec_p.at[g, i_]

    def own_line(piece, condition=None, own=None):
        ref, sem = piece[0](i, o)
        if own is not None:
            arrive(ref, sem, own)
        for e in range(1, inner_n):
            launch(ref, ref, sem, dev(o, turn_i(e), x, k), condition)

    def from_line(piece, d, condition=None):
        def act(there, valid, toward):
            valid = both(valid, condition)
            ref, sem = piece[0](i, there)
            arrive(ref, sem, valid)
            for e in range(1, inner_n):
                launch(ref, ref, sem, dev(o, turn_i(e), x, k), valid)

        by_distance(d, act)
        if d == outer_n - 1:
            launch(*pair(piece[1], i, k), partner, condition)

    def pair(block, i_, half):
        ref, sem = block(i_, half)
        return ref, ref, sem

    def from_pairs(piece, condition=None):
        for e in range(1, inner_n):
            for d in range(outer_n):
                arrive(*piece[0](turn_i(e), turn_o(d)), condition)
            launch(*pair(piece[1], turn_i(e), k), partner, condition)

    def from_partner(piece, condition=None):
        for e in range(inner_n):
            arrive(*piece[1](turn_i(e), other), condition)

    def kind(piece, block, which):
        return functools.partial(piece, which), functools.partial(block, which)

    lat_a, lat_b = kind(lat_piece, lat_block, 0), kind(lat_piece, lat_block, 1)
    rec = [kind(rec_piece, rec_block, g) for g in range(2)]
    own_line(lat_a)
    own_line(lat_b, extra)

    for b in range(blocks):

        @pl.when(blocks * k + b == o)
        def _():
            tok[b] = tok_in[...]

    sign_pick = spread(ATT_QK, 0, True)[NOPE_DIM:, LANES:].astype(bf16)
    depth = width // n
    rot_all[...] = (
        lax.dot_general(
            rot_down[...], sign_pick, (((0,), (0,)), ((), ())), preferred_element_type=f32
        )
        .astype(bf16)
        .reshape(n, depth, 2 * LANES)
    )

    own_line(rec[0], None, away)
    for j in range(2):
        for e in range(1, inner_n):
            launch(outs[j], *out_piece(j, i, o), dev(o, turn_i(e), x, k))
    own_line(rec[1], None, away)

    def gains(ref):
        wide = jnp.broadcast_to(ref[...], (8, ATT_QK))
        return jnp.dot(
            wide,
            spread(ATT_QK, 0, False),
            precision=lax.Precision.HIGHEST,
            preferred_element_type=f32,
        )[0:1]

    for j, target in enumerate((up_q, up_l, rate_ref, chain_gain_ref, mixer_gain_ref)):
        arrive(target, r_small.at[j], away)
    up_q[...] = jnp.dot(
        up_q[...],
        spread(heads * ATT_QK, hh * ATT_QK, True).astype(bf16),
        preferred_element_type=f32,
    ).astype(bf16)

    for j in range(2):
        out_w[j, i, o] = outs[j][...]

    def send_out(js=(0, 1)):
        for j in js:
            ref, sem = out_piece(j, i, o)
            for step, condition in ((1, right), (-1, left)):
                launch(outs[j], ref, sem, dev(o + step, i, x, k), condition)

    def relay_out(d, js=(0, 1)):
        for j in js:

            def act(there, valid, toward):
                ref, sem = out_piece(j, i, there)
                arrive(ref, sem, valid)
                if d < outer_n - 1:
                    onward = both(valid, right if toward > 0 else left)
                    launch(ref, ref, sem, dev(o + toward, i, x, k), onward)
                for e in range(1, inner_n):
                    launch(
                        ref, ref, sem, dev(o, turn_i(e), x, k), valid
                    )

            by_distance(d, act)


    def relay_tokens(c, there, valid, toward, last):
        ref, sem = stage.at[c, there], r_tok.at[c, there]
        arrive(ref, sem, valid)
        if not last:
            onward = both(valid, right if toward > 0 else left)
            launch(ref, ref, sem, dev(o + toward, i, x, k), onward)
        core, b = there // blocks, lax.rem(there, blocks)
        at = halves[c]
        target, sem = tok.at[b, t, :, at], r_deliver.at[c, b, t]
        launch(ref, target, sem, dev(o, i, 1 - x, core), valid)
        launch(ref, target, sem, partner, both(valid, core != k))

        @pl.when(both(valid, core == k))
        def _():
            tok[b, t, :, at] = stage[c, there]

    for d in range(1, outer_n):
        for c in range(2):
            by_distance(
                d,
                functools.partial(
                    lambda c, there, valid, toward: relay_tokens(
                        c, there, valid, toward, d == outer_n - 1
                    ),
                    c,
                ),
            )
        if d == 1:
            from_line(lat_a, 1)
            from_line(lat_b, 1, extra)
        if d == outer_n - 2:
            send_weights(0)
            for far_d in range(2, outer_n):
                from_line(lat_a, far_d)
                from_line(lat_b, far_d, extra)

    from_pairs(lat_a)
    from_pairs(lat_b, extra)

    for b in range(blocks):
        there = blocks * k + b
        for d in range(1, heads_n):
            q = lax.rem(t + d, heads_n)
            for c, at in enumerate(halves):
                arrive(tok.at[b, q, :, at], r_deliver.at[c, b, q], there != o)
        wide = jnp.concatenate([tok[b, q].astype(f32) for q in range(heads_n)], axis=0)
        scale = inverse_rms(wide, width)
        normed = (wide * scale * input_gain[...]).astype(bf16)
        for s in range(n):
            xs[s, b * rows : (b + 1) * rows, :] = normed[:, s * depth : (s + 1) * depth]

    def project(rhs, columns):
        def body(s, total):
            return total + jnp.dot(xs[s], rhs(s), preferred_element_type=f32)

        return lax.fori_loop(
            0, n, body, jnp.zeros((blocks * rows, columns), f32), unroll=n <= 8
        ).astype(bf16)

    from_partner(lat_a)
    from_partner(lat_b, extra)
    own_unit = x * q_units + o
    first = project(
        lambda s: jnp.concatenate([l_all[0, lax.rem(s, inner_n), s // inner_n].reshape(depth, LANES), rot_all[s]], axis=1),
        3 * LANES,
    )
    lat[own_unit] = first[:, :LANES]
    rotary = first[:, LANES:].astype(f32)

    @pl.when(extra)
    def _():
        lat[extra_unit] = project(lambda s: l_all[1, lax.rem(s, inner_n), s // inner_n].reshape(depth, LANES), LANES)

    def send_unit(unit, condition=None):
        for d in range(1, outer_n):
            launch(lat.at[unit], lat.at[unit], r_lat.at[unit], dev(turn_o(d), i, x, k), condition)
        launch(lat.at[unit], lat.at[unit], r_lat.at[unit], beside, condition)

    send_unit(own_unit)
    send_unit(extra_unit, extra)
    send_out((0,))
    for d in range(1, outer_n):
        from_line(rec[0], d)


    def relay_unit(there, valid, toward):
        unit = x * q_units + there
        arrive(lat.at[unit], r_lat.at[unit], valid)
        launch(lat.at[unit], lat.at[unit], r_lat.at[unit], beside, valid)

    for d in range(1, outer_n):
        by_distance(d, relay_unit)
    arrive(lat.at[extra_unit], r_lat.at[extra_unit], jnp.logical_not(extra))
    launch(
        lat.at[extra_unit],
        lat.at[extra_unit],
        r_lat.at[extra_unit],
        beside,
        jnp.logical_not(extra),
    )
    send_weights(1)
    send_out((1,))
    from_pairs(rec[0])
    relay_out(1, (0,))

    def shared(ref, sem):
        for e in range(1, inner_n):
            launch(ref, ref, sem, dev(o, turn_i(e), x, k))
        launch(ref, ref, sem, partner)

    def columns(s, mats_here):
        return jnp.concatenate([
                w_all[lax.rem(s, inner_n), s // inner_n, m].reshape(depth, LANES)
                for m in mats_here
            ], axis=1)

    from_partner(rec[0])
    vfb = project(lambda s: columns(s, (0, 1, 2)), 3 * LANES)
    value = [vfb[b * rows : (b + 1) * rows, :LANES] for b in range(blocks)]
    row = lax.broadcasted_iota(jnp.int32, (rows, rows), 0)
    col = lax.broadcasted_iota(jnp.int32, (rows, rows), 1)
    masks = (row >= col, row <= col)

    def direction(d):
        rate = rate_ref[d : d + 1, lane(hh)] / (rows * n)
        logit = vfb[:, (1 + d) * LANES : (2 + d) * LANES].astype(f32)
        key = rate * jax.nn.sigmoid(-logit)
        decay = jnp.log1p(-key)
        total = jnp.dot(
            jnp.where(masks[d], 1.0, 0.0),
            jnp.concatenate([decay[b * rows : (b + 1) * rows] for b in range(blocks)], axis=1),
            precision=lax.Precision.HIGHEST,
            preferred_element_type=f32,
        )
        keys, totals = [], []
        last = (rows - 1, 0)[d]
        for b in range(blocks):
            part = total[:, b * LANES : (b + 1) * LANES]
            full = part[last : last + 1, :]
            near = (key[b * rows : (b + 1) * rows] * jnp.exp(-part)).astype(bf16)
            state = lax.dot_general(
                value[b], near, (((0,), (0,)), ((), ())), preferred_element_type=f32
            )
            states[i, blocks * k + b, d] = (state * jnp.exp(full)).astype(bf16)
            logs[i, blocks * k + b, d] = jnp.broadcast_to(full, (8, LANES))
            keys.append(near)
            totals.append(part)
        return keys, totals

    near = [direction(d) for d in range(2)]

    def state_pieces(i_, k_):
        at = pl.ds(k_ * blocks, blocks)
        return (states.at[i_, at], r_state.at[i_, k_]), (logs.at[i_, at], r_log.at[i_, k_])

    for ref, sem in state_pieces(i, k):
        shared(ref, sem)

    for d in range(outer_n):
        unit = (1 - x) * q_units + turn_o(d)
        arrive(lat.at[unit], r_lat.at[unit])
    far_unit = outer_n + 1 - x
    arrive(lat.at[far_unit], r_lat.at[far_unit])

    cosines, sines = [], []
    for b in range(blocks):
        s = (blocks * k + b) * inner_n + i
        cb, sb = cos_block[pl.ds(s, 1), :], sin_block[pl.ds(s, 1), :]
        cosines.append(cb * cos_row[...] - sb * sin_row[...])
        sines.append(sb * cos_row[...] + cb * sin_row[...])
    cosine = jnp.concatenate(cosines, axis=0)
    sine = jnp.concatenate(sines, axis=0)

    def latent(first_unit, count, gain):
        wide = jnp.concatenate(
            [lat[u].astype(f32) for u in range(first_unit, first_unit + count)], axis=1
        )
        scaling = jnp.concatenate([gain[u : u + 1] for u in range(count)], axis=1)
        return (wide * inverse_rms(wide, count * LANES) * scaling).astype(bf16)

    def finish(plain, tail, swapped, gain):
        square = jnp.sum(plain * plain + tail * tail, axis=-1, keepdims=True)
        scale = lax.rsqrt(square / ATT_QK + norm_eps)
        turned = tail * gain[:, LANES : 2 * LANES] * cosine + swapped * gain[:, 2 * LANES :] * sine
        return jnp.concatenate(
            [(plain * scale * gain[:, :LANES]).astype(bf16), (turned * scale).astype(bf16)], axis=1
        )

    pairs = jnp.dot(
        latent(q_units, outer_n, latent_gain), up_l[...], preferred_element_type=f32
    ).astype(bf16)
    kv[i, k, :, : 2 * LANES] = finish(
        pairs[:, :LANES].astype(f32), rotary[:, :LANES], rotary[:, LANES:], gains(key_gain)
    )
    kv[i, k, :, 2 * LANES :] = pairs[:, LANES:]

    shared(kv.at[i, k], r_kv.at[i, k])

    attend_q = (
        jnp.dot(latent(0, q_units, query_latent_gain), up_q[...], preferred_element_type=f32)
        .astype(bf16)
        .astype(f32)
    )
    query = finish(
        attend_q[:, :LANES],
        attend_q[:, LANES : 2 * LANES],
        attend_q[:, 2 * LANES :],
        gains(query_gain),
    )


    scale = ATT_QK ** (-0.5) * 1.4426950408889634

    def attend(carry, i_, k_):
        numer, denom = carry
        score = against(query, kv[i_, k_, :, : 2 * LANES])
        weight = jnp.exp2(score * scale)
        numer += jnp.dot(
            weight.astype(bf16), kv[i_, k_, :, 2 * LANES :], preferred_element_type=f32
        )
        return numer, denom + jnp.sum(weight, axis=-1, keepdims=True)

    carry = (jnp.zeros((blocks * rows, LANES), f32), jnp.zeros((blocks * rows, 1), f32))
    carry = attend(carry, i, k)
    arrive(kv.at[i, other], r_kv.at[i, other])
    carry = attend(carry, i, other)
    for d in range(1, outer_n):
        from_line(rec[1], d)
    relay_out(1, (1,))
    relay_out(2, (0,))

    def relay_pair(ref, sem):
        arrive(ref, sem)
        launch(ref, ref, sem, partner)

    for e in range(1, inner_n):
        relay_pair(kv.at[turn_i(e), k], r_kv.at[turn_i(e), k])
    for e in range(1, inner_n):
        for ref, sem in state_pieces(turn_i(e), k):
            relay_pair(ref, sem)
    from_pairs(rec[1])
    relay_out(2, (1,))
    relay_out(3, (0,))
    for e in range(1, inner_n):
        there = turn_i(e)
        carry = attend(carry, there, k)
        arrive(kv.at[there, other], r_kv.at[there, other])
        carry = attend(carry, there, other)
    rows_out = carry[0] / carry[1]
    attend_mixed = (
        rows_out * inverse_rms(rows_out, LANES) * mixer_gain_ref[:, lane(hh)]
    ).astype(bf16)

    from_partner(rec[1])
    qg = project(lambda s: columns(s, (3, 4)), 2 * LANES).astype(f32)
    for e in range(inner_n):
        for k_ in (k, other):
            if e or k_ is other:
                for ref, sem in state_pieces(turn_i(e), k_):
                    if k_ is other:
                        arrive(ref, sem)

    def forward(s, state):
        i_, o_ = lax.rem(s, inner_n), s // inner_n
        return state * jnp.exp(logs[i_, o_, 0, 0:1, :]) + states[i_, o_, 0].astype(f32)

    def backward(j, state):
        s = n - 1 - j
        i_, o_ = lax.rem(s, inner_n), s // inner_n
        return state * jnp.exp(logs[i_, o_, 1, 0:1, :]) + states[i_, o_, 1].astype(f32)

    nothing = jnp.zeros((LANES, LANES), f32)
    for b in range(blocks):
        there = blocks * k + b
        s = there * inner_n + i
        incoming = (
            lax.fori_loop(0, s, forward, nothing).astype(bf16),
            lax.fori_loop(0, n - 1 - s, backward, nothing).astype(bf16),
        )
        at = slice(b * rows, (b + 1) * rows)
        total = jnp.zeros((rows, LANES), f32)
        within = jnp.zeros((rows, rows), f32)
        for d in range(2):
            keys, totals = near[d]
            probe = (qg[at, :LANES] * jnp.exp(totals[b])).astype(bf16)
            within += jnp.where(masks[d], against(probe, keys[b]), 0.0)
            total += against(probe, incoming[d])
        total += jnp.dot(within.astype(bf16), value[b], preferred_element_type=f32)
        gate = qg[at, LANES:]
        scaled = total * inverse_rms(total, LANES) * chain_gain_ref[:, lane(hh)]
        mix_send[b, :, :LANES] = (scaled * (gate * jax.nn.sigmoid(gate))).astype(bf16)
        mix_send[b, :, LANES:] = attend_mixed[at]
        home = there == o
        launch(
            mix_send.at[b],
            mix_recv.at[hh],
            r_mix.at[hh],
            dev(there, i, x, o // heads),
            jnp.logical_not(home),
        )

        @pl.when(home)
        def _():
            mix_recv[hh] = mix_send[b]

    relay_out(3, (1,))

    for h in range(heads):
        arrive(mix_recv.at[h], r_mix.at[h], heads * k + h != o)
    col_n = out_w.shape[4]
    span = inner_n * col_n
    own_rows = 2 * part_rows
    order = (o, o + 1 - 2 * lax.rem(o, 2), turn_o(2), outer_n - 1 - o)
    assert outer_n == len(order)

    def rows_of(x_):
        at = pl.ds(pl.multiple_of(x_ * own_rows, own_rows), own_rows)
        return [
            jnp.concatenate(
                [mix_recv[h, at, p * LANES : (p + 1) * LANES] for h in range(heads)], axis=1
            )
            for p in range(2)
        ]

    def partial(target, c, rows_here):
        for e in range(inner_n):
            product = jnp.dot(
                rows_here[0], out_w[0, e, order[c]], preferred_element_type=f32
            ) + jnp.dot(rows_here[1], out_w[1, e, order[c]], preferred_element_type=f32)
            for q in range(2):
                target[c, q, :, e * col_n : (e + 1) * col_n] = product[
                    q * part_rows : (q + 1) * part_rows
                ]

    rows_far, rows_near = rows_of(1 - x), rows_of(x)
    def cross(c):
        arrive(got_far.at[c], r_sum.at[0, c])
        send_x[c] = (part_far[c, k] + got_far[c].astype(f32)).astype(bf16)
        launch(send_x.at[c], got_x.at[c], r_sum.at[1, c], beside)

    for c in range(outer_n):
        for j in range(2):
            for e in range(1, inner_n):
                arrive(*out_piece(j, turn_i(e), order[c]))
        partial(part_far, c, rows_far)
        send_far[c] = part_far[c, other].astype(bf16)
        launch(send_far.at[c], got_far.at[c], r_sum.at[0, c], partner)
        if c:
            cross(c - 1)
        partial(part_near, c, rows_near)
        send_near[c] = part_near[c, other].astype(bf16)
        launch(send_near.at[c], got_near.at[c], r_sum.at[2, c], partner)
    cross(outer_n - 1)
    for c in range(outer_n):
        arrive(got_near.at[c], r_sum.at[2, c])
        arrive(got_x.at[c], r_sum.at[1, c])
        out_ref[:, lane(order[c], span)] = (
            part_near[c, k] + got_near[c].astype(f32) + got_x[c].astype(f32)
        )
    drain()
    needed.append(used[0])


def on_device(
    tokens,
    input_gain,
    chain_query,
    forward_gate,
    backward_gate,
    chain_value,
    output_gate,
    forget_rate,
    chain_gain,
    query_down,
    latent_down,
    rotary_down,
    query_latent_gain,
    latent_gain,
    query_up,
    latent_up,
    query_head_gain,
    key_head_gain,
    mixer_gain,
    chain_out,
    attend_out,
):
    n, heads_n = lax.axis_size("sp"), lax.axis_size("tp")
    rows, width = tokens.shape
    depth = chain_query.shape[0]
    heads = query_up.shape[1] // ATT_QK
    outer_n = 2 * heads
    inner_n = n // outer_n
    blocks = outer_n // 2
    half = depth // 2
    units = (query_down.shape[1] + latent_down.shape[1]) // LANES
    part = rows // heads_n
    out_cols = n * chain_out.shape[1]

    inverse = rope_theta ** (-np.arange(0, ROPE_DIM, 2) / ROPE_DIM)

    def table(positions):
        angles = np.tile(positions[:, None] * inverse, (1, 2))
        pad = ((0, 0), (0, LANES - ROPE_DIM))
        return [jnp.asarray(np.pad(f(angles), pad), f32) for f in (np.cos, np.sin)]

    in_row = table(np.arange(rows, dtype=np.float64))
    in_block = table(np.arange(n, dtype=np.float64) * rows)

    def halves(w):
        return w.reshape(2, half, w.shape[1])

    operands = (
        tokens.reshape(heads_n, part, width),
        *[
            halves(w)
            for w in (
                chain_value,
                forward_gate,
                backward_gate,
                chain_query,
                output_gate,
                query_down,
                latent_down,
            )
        ],
        rotary_down.T,
        query_up,
        latent_up,
        chain_out,
        attend_out,
        forget_rate,
        chain_gain[None],
        mixer_gain[None],
        input_gain[None],
        query_latent_gain.reshape(-1, LANES),
        latent_gain.reshape(-1, LANES),
        query_head_gain[None],
        key_head_gain[None],
        *in_row,
        *in_block,
    )
    dma = pltpu.SemaphoreType.DMA
    vmem = pl.BlockSpec(memory_space=pltpu.VMEM)
    tall = blocks * rows
    needed = []
    hbm = pl.BlockSpec(memory_space=pltpu.HBM)
    big = operands[:13]

    def build(sends):
      return pl.pallas_call(
        functools.partial(mixer_kernel, n, heads_n, heads, sends, needed),
        out_shape=jax.ShapeDtypeStruct((part, out_cols), f32),
        in_specs=[hbm] * len(big) + [vmem] * (len(operands) - len(big)),
        out_specs=vmem,
        scratch_shapes=[
            pltpu.VMEM((2, outer_n, part, width // 2), bf16),
            pltpu.VMEM((blocks, heads_n, part, width), bf16),
            pltpu.VMEM((n, tall, depth), bf16),
            pltpu.VMEM((inner_n, outer_n, 5, 2, half, LANES), bf16),
            pltpu.VMEM((2, inner_n, outer_n, 2, half, LANES), bf16),
            pltpu.VMEM((n, depth, 2 * LANES), bf16),
            pltpu.VMEM((units, tall, LANES), bf16),
            pltpu.VMEM(forget_rate.shape, f32),
            pltpu.VMEM((1,) + chain_gain.shape, f32),
            pltpu.VMEM((1,) + mixer_gain.shape, f32),
            pltpu.VMEM(query_up.shape, bf16),
            pltpu.VMEM((latent_up.shape[0], 2 * LANES), bf16),
            pltpu.VMEM((inner_n, 2, tall, 3 * LANES), bf16),
            pltpu.VMEM((inner_n, outer_n, 2, LANES, LANES), bf16),
            pltpu.VMEM((inner_n, outer_n, 2, 8, LANES), f32),
            pltpu.VMEM((blocks, rows, 2 * LANES), bf16),
            pltpu.VMEM((heads, rows, 2 * LANES), bf16),
            pltpu.VMEM((2, inner_n, outer_n) + chain_out.shape, bf16),
            pltpu.VMEM((outer_n, 2, part, out_cols // outer_n), f32),
            pltpu.VMEM((outer_n, 2, part, out_cols // outer_n), f32),
            pltpu.VMEM((outer_n, part, out_cols // outer_n), bf16),
            pltpu.VMEM((outer_n, part, out_cols // outer_n), bf16),
            pltpu.VMEM((outer_n, part, out_cols // outer_n), bf16),
            pltpu.VMEM((outer_n, part, out_cols // outer_n), bf16),
            pltpu.VMEM((outer_n, part, out_cols // outer_n), bf16),
            pltpu.VMEM((outer_n, part, out_cols // outer_n), bf16),
            dma((sends,)),
            dma((2, outer_n)),
            dma((2, blocks, heads_n)),
            dma((2, inner_n, outer_n)),
            dma((2, inner_n)),
            dma((2, inner_n, outer_n)),
            dma((2, inner_n)),
            dma((5,)),
            dma((units,)),
            dma((inner_n, 2)),
            dma((inner_n, 2)),
            dma((inner_n, 2)),
            dma((heads,)),
            dma((2, inner_n, outer_n)),
            dma((3, outer_n)),
        ]
        + [pltpu.VMEM(a.shape, a.dtype) for a in big]
        + [dma((len(big),))],
        compiler_params=pltpu.CompilerParams(
            collective_id=0, has_side_effects=True, vmem_limit_bytes=VMEM_LIMIT
        ),
      )

    jax.eval_shape(build(200 + 30 * n), *operands)
    held = [pltpu.with_memory_space_constraint(a, pltpu.HBM) for a in operands]
    return build(needed[0])(*held)


def solution(mesh):
    placed = (
        P("sp", None),
        P(),
        P("sp", "tp"),
        P("sp", "tp"),
        P("sp", "tp"),
        P("sp", "tp"),
        P("sp", "tp"),
        P(None, "tp"),
        P("tp"),
        P("sp", None),
        P("sp", None),
        P(),
        P(),
        P(),
        P(None, "tp"),
        P(None, "tp"),
        P(),
        P(),
        P("tp"),
        P("tp", "sp"),
        P("tp", "sp"),
    )
    return jax.shard_map(
        on_device, mesh=mesh, in_specs=placed, out_specs=P(("sp", "tp"), None), check_vma=False
    )
```

```python
import functools

import jax
import jax.numpy as jnp
import numpy as np
from jax import lax
from jax.experimental import pallas as pl
from jax.experimental.pallas import tpu as pltpu
from jax.sharding import PartitionSpec as P

LANES = 128
RING = 64
NOPE_DIM = 128
ROPE_DIM = 64
ATT_QK = 192
HALF = ROPE_DIM // 2

norm_eps = 1e-06
rope_theta = 10000.0
MESH = pl.DeviceIdType.MESH
VMEM_LIMIT = 48 * 1024 * 1024
f32 = jnp.float32
bf16 = jnp.bfloat16


def run_if(condition, act):
    if condition is None:
        act()
    else:
        pl.when(condition)(act)


def both(a, b):
    if a is None:
        return b
    if b is None:
        return a
    return jnp.logical_and(a, b)


def against(a, b):
    return lax.dot_general(a, b, (((1,), (1,)), ((), ())), preferred_element_type=f32)


def inverse_rms(values, size):
    return lax.rsqrt(jnp.sum(values * values, axis=-1, keepdims=True) / size + norm_eps)


def spread(count, start, signed):
    row = lax.broadcasted_iota(jnp.int32, (count, 3 * LANES), 0) - start
    col = lax.broadcasted_iota(jnp.int32, (count, 3 * LANES), 1)
    straight = (col < ATT_QK) & (row == col)
    at = col - 2 * LANES
    low = (at >= 0) & (at < HALF) & (row == NOPE_DIM + HALF + at)
    high = (at >= HALF) & (at < ROPE_DIM) & (row == NOPE_DIM + at - HALF)
    return (
        jnp.where(straight, 1.0, 0.0)
        + jnp.where(low, -1.0 if signed else 1.0, 0.0)
        + jnp.where(high, 1.0, 0.0)
    )


def mixer_kernel(n, heads_n, heads, sends, needed, *refs):
    count = 13
    far, near_by = refs[:count], refs[-count - 1 : -1]
    fetched = refs[-1]
    (
        tok_in,
        wv,
        wf,
        wb,
        wq,
        wg,
        q_down,
        l_down,
        rot_down,
        query_up,
        latent_up,
        chain_out,
        attend_out,
    ) = near_by
    (
        rate_in,
        chain_gain_in,
        mixer_gain_in,
        input_gain,
        query_latent_gain,
        latent_gain,
        query_gain,
        key_gain,
        cos_row,
        sin_row,
        cos_block,
        sin_block,
        out_ref,
        stage,
        tok,
        xs,
        w_all,
        l_all,
        rot_all,
        lat,
        rate_ref,
        chain_gain_ref,
        mixer_gain_ref,
        up_q,
        up_l,
        kv,
        states,
        logs,
        mix_send,
        mix_recv,
        out_w,
        part_far,
        part_near,
        send_far,
        send_near,
        got_far,
        got_near,
        send_x,
        got_x,
        ssem,
        r_tok,
        r_deliver,
        r_lat_w,
        r_lat_p,
        r_rec_w,
        r_rec_p,
        r_small,
        r_lat,
        r_kv,
        r_state,
        r_log,
        r_mix,
        r_out,
        r_sum,
    ) = refs[count : -count - 1]
    mats = (wv, wf, wb, wq, wg)
    groups = ((0, 3), (3, 2))
    outer_n = 2 * heads
    inner_n = n // outer_n
    blocks = outer_n // 2
    part_rows, width = tok_in.shape[1:]
    chunk = width // 2
    rows = part_rows * heads_n
    q_units = q_down.shape[2] // LANES

    me = lax.axis_index("sp")
    t = lax.axis_index("tp")
    o, i = me // inner_n, lax.rem(me, inner_n)
    x, k = t // 2, lax.rem(t, 2)
    other = 1 - k
    at_home = (o // heads) == k
    away = jnp.logical_not(at_home)
    hh = lax.rem(o, heads)

    def dev(o_, i_, x_, k_):
        return {"sp": o_ * inner_n + i_, "tp": x_ * 2 + k_}

    def turn_o(d):
        return lax.rem(o + d, outer_n)

    def turn_i(d):
        return lax.rem(i + d, inner_n)

    def lane(index, size=LANES):
        return pl.ds(pl.multiple_of(index * size, LANES), size)

    peers = [dev(turn_o(d), i, x, r) for d in range(1, outer_n) for r in range(2)]
    peers += [dev(o, turn_i(d), x, k) for d in range(1, inner_n)]
    peers += [{"sp": me, "tp": lax.rem(t + d, heads_n)} for d in range(1, heads_n)]
    fetches = [pltpu.make_async_copy(far[j], near_by[j], fetched.at[j]) for j in range(count)]
    for fetch in fetches:
        fetch.start()
    barrier = pltpu.get_barrier_semaphore()
    for peer in peers:
        pl.semaphore_signal(barrier, inc=1, device_id=peer, device_id_type=MESH)
    pl.semaphore_wait(barrier, len(peers))

    pending, used, shared_slots = [], [0], set()
    ring = min(sends, RING)

    def copy(src, dst, send_sem, recv_sem, device):
        return pltpu.make_async_remote_copy(
            src_ref=src,
            dst_ref=dst,
            send_sem=send_sem,
            recv_sem=recv_sem,
            device_id=device,
            device_id_type=MESH,
        )

    def launch(src, dst, recv_sem, device, condition=None, index=None):
        if index is None:
            if used[0] < ring:
                index = used[0]
                used[0] += 1
            else:
                at = next(a for a, entry in enumerate(pending) if entry[2] not in shared_slots)
                finished, finish_send, index = pending.pop(at)
                run_if(finished, finish_send)

        def make():
            return copy(src, dst, ssem.at[index], recv_sem, device)

        run_if(condition, lambda: make().start())
        pending.append((condition, lambda: make().wait_send(), index))
        return index

    def by_distance(d, act):
        for there, toward in ((o - d, 1), (o + d, -1)):
            valid = (there >= 0) & (there < outer_n)
            act(jnp.clip(there, 0, outer_n - 1), valid, toward)

    def drain():
        for condition, finish_send, _ in pending:
            run_if(condition, finish_send)

    def arrive(dst, recv_sem, condition=None):
        run_if(
            condition,
            lambda: copy(dst, dst, ssem.at[0], recv_sem, dev(o, i, x, other)).wait_recv(),
        )

    partner = dev(o, i, x, other)
    beside = dev(o, i, 1 - x, k)

    right, left = o + 1 < outer_n, o > 0
    halves = [slice(c * chunk, (c + 1) * chunk) for c in range(2)]
    fetches[0].wait()
    for c, at in enumerate(halves):
        for step, condition in ((1, right), (-1, left)):
            launch(
                tok_in.at[t, :, at],
                stage.at[c, o],
                r_tok.at[c, o],
                dev(o + step, i, x, k),
                condition,
            )

    is_q, is_l = x == 0, x != 0
    extra_o, extra_unit = 1 + x, outer_n + x
    extra = o == extra_o
    for fetch in fetches[6:8]:
        fetch.wait()
    for d in range(1, outer_n):
        there, index = turn_o(d), None
        for source, condition in ((q_down, is_q), (l_down, is_l)):
            index = launch(
                source.at[k, :, lane(there)],
                l_all.at[0, i, o, k],
                r_lat_w.at[0, i, o],
                dev(there, i, x, k),
                condition,
                index,
            )
        shared_slots.add(index)
    launch(
        q_down.at[k, :, lane(extra_unit)],
        l_all.at[1, i, o, k],
        r_lat_w.at[1, i, o],
        dev(extra_o, i, x, k),
        jnp.logical_not(extra),
    )
    for fetch in fetches[1:6] + fetches[8:]:
        fetch.wait()

    def send_weights(g):
        first, count = groups[g]
        for m in range(first, first + count):
            for h in range(heads):
                there = heads * k + h
                for r in range(2):
                    launch(
                        mats[m].at[r, :, h * LANES : (h + 1) * LANES],
                        w_all.at[i, o, m, r],
                        r_rec_w.at[g, i, o],
                        dev(there, i, x, r),
                        there != o,
                    )

    def send_home_weights(g):
        first, count = groups[g]
        for m in range(first, first + count):
            launch(
                mats[m].at[other, :, lane(hh)],
                w_all.at[i, o, m, other],
                r_rec_w.at[g, i, o],
                partner,
                at_home,
            )

    def out_piece(j, i_, o_):
        return out_w.at[j, i_, o_], r_out.at[j, i_, o_]

    outs = (chain_out, attend_out)
    send_home_weights(0)
    for j, (source, target) in enumerate(
        (
            (query_up, up_q),
            (latent_up.at[:, lane(hh, 2 * LANES)], up_l),
            (rate_in, rate_ref),
            (chain_gain_in, chain_gain_ref),
            (mixer_gain_in, mixer_gain_ref),
        )
    ):
        launch(source, target, r_small.at[j], partner, at_home)
    send_home_weights(1)

    @pl.when(is_q)
    def _():
        l_all[0, i, o, k] = q_down[k, :, lane(o)]

    @pl.when(is_l)
    def _():
        l_all[0, i, o, k] = l_down[k, :, lane(o)]

    @pl.when(extra)
    def _():
        l_all[1, i, o, k] = q_down[k, :, lane(extra_unit)]

    @pl.when(at_home)
    def _():
        for m in range(len(mats)):
            w_all[i, o, m, k] = mats[m][k, :, lane(hh)]
        up_q[...] = query_up[...]
        up_l[...] = latent_up[:, lane(hh, 2 * LANES)]
        rate_ref[...] = rate_in[...]
        chain_gain_ref[...] = chain_gain_in[...]
        mixer_gain_ref[...] = mixer_gain_in[...]

    def lat_piece(slot, i_, o_):
        return l_all.at[slot, i_, o_, k], r_lat_w.at[slot, i_, o_]

    def lat_block(slot, i_, half):
        return l_all.at[slot, i_, :, half], r_lat_p.at[slot, i_]

    def rec_piece(g, i_, o_):
        first, count = groups[g]
        return w_all.at[i_, o_, first : first + count, k], r_rec_w.at[g, i_, o_]

    def rec_block(g, i_, half):
        first, count = groups[g]
        return w_all.at[i_, :, first : first + count, half], r_rec_p.at[g, i_]

    def own_line(piece, condition=None, own=None):
        ref, sem = piece[0](i, o)
        if own is not None:
            arrive(ref, sem, own)
        for e in range(1, inner_n):
            launch(ref, ref, sem, dev(o, turn_i(e), x, k), condition)

    def from_line(piece, d, condition=None):
        def act(there, valid, toward):
            valid = both(valid, condition)
            ref, sem = piece[0](i, there)
            arrive(ref, sem, valid)
            for e in range(1, inner_n):
                launch(ref, ref, sem, dev(o, turn_i(e), x, k), valid)

        by_distance(d, act)
        if d == outer_n - 1:
            launch(*pair(piece[1], i, k), partner, condition)

    def pair(block, i_, half):
        ref, sem = block(i_, half)
        return ref, ref, sem

    def from_pairs(piece, condition=None):
        for e in range(1, inner_n):
            for d in range(outer_n):
                arrive(*piece[0](turn_i(e), turn_o(d)), condition)
            launch(*pair(piece[1], turn_i(e), k), partner, condition)

    def from_partner(piece, condition=None):
        for e in range(inner_n):
            arrive(*piece[1](turn_i(e), other), condition)

    def kind(piece, block, which):
        return functools.partial(piece, which), functools.partial(block, which)

    lat_a, lat_b = kind(lat_piece, lat_block, 0), kind(lat_piece, lat_block, 1)
    rec = [kind(rec_piece, rec_block, g) for g in range(2)]
    own_line(lat_a)
    own_line(lat_b, extra)

    for b in range(blocks):

        @pl.when(blocks * k + b == o)
        def _():
            tok[b] = tok_in[...]

    sign_pick = spread(ATT_QK, 0, True)[NOPE_DIM:, LANES:].astype(bf16)
    depth = width // n
    rot_all[...] = (
        lax.dot_general(
            rot_down[...], sign_pick, (((0,), (0,)), ((), ())), preferred_element_type=f32
        )
        .astype(bf16)
        .reshape(n, depth, 2 * LANES)
    )

    own_line(rec[0], None, away)
    for j in range(2):
        for e in range(1, inner_n):
            launch(outs[j], *out_piece(j, i, o), dev(o, turn_i(e), x, k))
    own_line(rec[1], None, away)

    def gains(ref):
        wide = jnp.broadcast_to(ref[...], (8, ATT_QK))
        return jnp.dot(
            wide,
            spread(ATT_QK, 0, False),
            precision=lax.Precision.HIGHEST,
            preferred_element_type=f32,
        )[0:1]

    for j, target in enumerate((up_q, up_l, rate_ref, chain_gain_ref, mixer_gain_ref)):
        arrive(target, r_small.at[j], away)
    up_q[...] = jnp.dot(
        up_q[...],
        spread(heads * ATT_QK, hh * ATT_QK, True).astype(bf16),
        preferred_element_type=f32,
    ).astype(bf16)

    for j in range(2):
        out_w[j, i, o] = outs[j][...]

    def send_out(js=(0, 1)):
        for j in js:
            ref, sem = out_piece(j, i, o)
            for step, condition in ((1, right), (-1, left)):
                launch(outs[j], ref, sem, dev(o + step, i, x, k), condition)

    def relay_out(d, js=(0, 1)):
        for j in js:

            def act(there, valid, toward):
                ref, sem = out_piece(j, i, there)
                arrive(ref, sem, valid)
                if d < outer_n - 1:
                    onward = both(valid, right if toward > 0 else left)
                    launch(ref, ref, sem, dev(o + toward, i, x, k), onward)
                for e in range(1, inner_n):
                    launch(
                        ref, ref, sem, dev(o, turn_i(e), x, k), valid
                    )

            by_distance(d, act)


    def relay_tokens(c, there, valid, toward, last):
        ref, sem = stage.at[c, there], r_tok.at[c, there]
        arrive(ref, sem, valid)
        if not last:
            onward = both(valid, right if toward > 0 else left)
            launch(ref, ref, sem, dev(o + toward, i, x, k), onward)
        core, b = there // blocks, lax.rem(there, blocks)
        at = halves[c]
        target, sem = tok.at[b, t, :, at], r_deliver.at[c, b, t]
        launch(ref, target, sem, dev(o, i, 1 - x, core), valid)
        launch(ref, target, sem, partner, both(valid, core != k))

        @pl.when(both(valid, core == k))
        def _():
            tok[b, t, :, at] = stage[c, there]

    for d in range(1, outer_n):
        for c in range(2):
            by_distance(
                d,
                functools.partial(
                    lambda c, there, valid, toward: relay_tokens(
                        c, there, valid, toward, d == outer_n - 1
                    ),
                    c,
                ),
            )
        if d == 1:
            from_line(lat_a, 1)
            from_line(lat_b, 1, extra)
        if d == outer_n - 2:
            send_weights(0)
            for far_d in range(2, outer_n):
                from_line(lat_a, far_d)
                from_line(lat_b, far_d, extra)

    from_pairs(lat_a)
    from_pairs(lat_b, extra)

    for b in range(blocks):
        there = blocks * k + b
        for d in range(1, heads_n):
            q = lax.rem(t + d, heads_n)
            for c, at in enumerate(halves):
                arrive(tok.at[b, q, :, at], r_deliver.at[c, b, q], there != o)
        wide = jnp.concatenate([tok[b, q].astype(f32) for q in range(heads_n)], axis=0)
        scale = inverse_rms(wide, width)
        normed = (wide * scale * input_gain[...]).astype(bf16)
        for s in range(n):
            xs[s, b * rows : (b + 1) * rows, :] = normed[:, s * depth : (s + 1) * depth]

    def project(rhs, columns):
        def body(s, total):
            return total + jnp.dot(xs[s], rhs(s), preferred_element_type=f32)

        return lax.fori_loop(
            0, n, body, jnp.zeros((blocks * rows, columns), f32), unroll=n <= 8
        ).astype(bf16)

    from_partner(lat_a)
    from_partner(lat_b, extra)
    own_unit = x * q_units + o
    first = project(
        lambda s: jnp.concatenate([l_all[0, lax.rem(s, inner_n), s // inner_n].reshape(depth, LANES), rot_all[s]], axis=1),
        3 * LANES,
    )
    lat[own_unit] = first[:, :LANES]
    rotary = first[:, LANES:].astype(f32)

    @pl.when(extra)
    def _():
        lat[extra_unit] = project(lambda s: l_all[1, lax.rem(s, inner_n), s // inner_n].reshape(depth, LANES), LANES)

    def send_unit(unit, condition=None):
        for d in range(1, outer_n):
            launch(lat.at[unit], lat.at[unit], r_lat.at[unit], dev(turn_o(d), i, x, k), condition)
        launch(lat.at[unit], lat.at[unit], r_lat.at[unit], beside, condition)

    send_unit(own_unit)
    send_unit(extra_unit, extra)
    send_out((0,))
    for d in range(1, outer_n):
        from_line(rec[0], d)


    def relay_unit(there, valid, toward):
        unit = x * q_units + there
        arrive(lat.at[unit], r_lat.at[unit], valid)
        launch(lat.at[unit], lat.at[unit], r_lat.at[unit], beside, valid)

    for d in range(1, outer_n):
        by_distance(d, relay_unit)
    arrive(lat.at[extra_unit], r_lat.at[extra_unit], jnp.logical_not(extra))
    launch(
        lat.at[extra_unit],
        lat.at[extra_unit],
        r_lat.at[extra_unit],
        beside,
        jnp.logical_not(extra),
    )
    send_weights(1)
    send_out((1,))
    from_pairs(rec[0])
    relay_out(1, (0,))

    def shared(ref, sem):
        for e in range(1, inner_n):
            launch(ref, ref, sem, dev(o, turn_i(e), x, k))
        launch(ref, ref, sem, partner)

    def columns(s, mats_here):
        return jnp.concatenate([
                w_all[lax.rem(s, inner_n), s // inner_n, m].reshape(depth, LANES)
                for m in mats_here
            ], axis=1)

    from_partner(rec[0])
    vfb = project(lambda s: columns(s, (0, 1, 2)), 3 * LANES)
    value = [vfb[b * rows : (b + 1) * rows, :LANES] for b in range(blocks)]
    row = lax.broadcasted_iota(jnp.int32, (rows, rows), 0)
    col = lax.broadcasted_iota(jnp.int32, (rows, rows), 1)
    masks = (row >= col, row <= col)

    def direction(d):
        rate = rate_ref[d : d + 1, lane(hh)] / (rows * n)
        logit = vfb[:, (1 + d) * LANES : (2 + d) * LANES].astype(f32)
        key = rate * jax.nn.sigmoid(-logit)
        decay = jnp.log1p(-key)
        total = jnp.dot(
            jnp.where(masks[d], 1.0, 0.0),
            jnp.concatenate([decay[b * rows : (b + 1) * rows] for b in range(blocks)], axis=1),
            precision=lax.Precision.HIGHEST,
            preferred_element_type=f32,
        )
        keys, totals = [], []
        last = (rows - 1, 0)[d]
        for b in range(blocks):
            part = total[:, b * LANES : (b + 1) * LANES]
            full = part[last : last + 1, :]
            near = (key[b * rows : (b + 1) * rows] * jnp.exp(-part)).astype(bf16)
            state = lax.dot_general(
                value[b], near, (((0,), (0,)), ((), ())), preferred_element_type=f32
            )
            states[i, blocks * k + b, d] = (state * jnp.exp(full)).astype(bf16)
            logs[i, blocks * k + b, d] = jnp.broadcast_to(full, (8, LANES))
            keys.append(near)
            totals.append(part)
        return keys, totals

    near = [direction(d) for d in range(2)]

    def state_pieces(i_, k_):
        at = pl.ds(k_ * blocks, blocks)
        return (states.at[i_, at], r_state.at[i_, k_]), (logs.at[i_, at], r_log.at[i_, k_])

    for ref, sem in state_pieces(i, k):
        shared(ref, sem)

    for d in range(outer_n):
        unit = (1 - x) * q_units + turn_o(d)
        arrive(lat.at[unit], r_lat.at[unit])
    far_unit = outer_n + 1 - x
    arrive(lat.at[far_unit], r_lat.at[far_unit])

    cosines, sines = [], []
    for b in range(blocks):
        s = (blocks * k + b) * inner_n + i
        cb, sb = cos_block[pl.ds(s, 1), :], sin_block[pl.ds(s, 1), :]
        cosines.append(cb * cos_row[...] - sb * sin_row[...])
        sines.append(sb * cos_row[...] + cb * sin_row[...])
    cosine = jnp.concatenate(cosines, axis=0)
    sine = jnp.concatenate(sines, axis=0)

    def latent(first_unit, count, gain):
        wide = jnp.concatenate(
            [lat[u].astype(f32) for u in range(first_unit, first_unit + count)], axis=1
        )
        scaling = jnp.concatenate([gain[u : u + 1] for u in range(count)], axis=1)
        return (wide * inverse_rms(wide, count * LANES) * scaling).astype(bf16)

    def finish(plain, tail, swapped, gain):
        square = jnp.sum(plain * plain + tail * tail, axis=-1, keepdims=True)
        scale = lax.rsqrt(square / ATT_QK + norm_eps)
        turned = tail * gain[:, LANES : 2 * LANES] * cosine + swapped * gain[:, 2 * LANES :] * sine
        return (plain * scale * gain[:, :LANES]).astype(bf16), turned * scale

    pairs = jnp.dot(
        latent(q_units, outer_n, latent_gain), up_l[...], preferred_element_type=f32
    ).astype(bf16)
    key_plain, key_turned = finish(
        pairs[:, :LANES].astype(f32), rotary[:, :LANES], rotary[:, LANES:], gains(key_gain)
    )
    assert blocks * ROPE_DIM == LANES
    packed = jnp.zeros((rows, LANES), f32)
    for b in range(blocks):
        at = slice(b * rows, (b + 1) * rows)
        kv[i, k, b] = key_plain[at]
        kv[i, k, blocks + b] = pairs[at, LANES:]
        part = key_turned[at]
        packed += pltpu.roll(part, b * ROPE_DIM, axis=1) if b else part
    kv[i, k, 2 * blocks] = packed.astype(bf16)

    shared(kv.at[i, k], r_kv.at[i, k])

    attend_q = (
        jnp.dot(latent(0, q_units, query_latent_gain), up_q[...], preferred_element_type=f32)
        .astype(bf16)
        .astype(f32)
    )
    query_plain, query_turned = finish(
        attend_q[:, :LANES],
        attend_q[:, LANES : 2 * LANES],
        attend_q[:, 2 * LANES :],
        gains(query_gain),
    )
    queries = [
        jnp.concatenate(
            [
                query_plain,
                (pltpu.roll(query_turned, b * ROPE_DIM, axis=1) if b else query_turned).astype(bf16),
            ],
            axis=1,
        )
        for b in range(blocks)
    ]


    scale = ATT_QK ** (-0.5) * 1.4426950408889634

    def attend(carry, i_, k_):
        numer, denom = carry
        for b in range(blocks):
            key = jnp.concatenate([kv[i_, k_, b], kv[i_, k_, 2 * blocks]], axis=1)
            weight = jnp.exp2(against(queries[b], key) * scale)
            numer += jnp.dot(
                weight.astype(bf16), kv[i_, k_, blocks + b], preferred_element_type=f32
            )
            denom += jnp.sum(weight, axis=-1, keepdims=True)
        return numer, denom

    carry = (jnp.zeros((blocks * rows, LANES), f32), jnp.zeros((blocks * rows, 1), f32))
    carry = attend(carry, i, k)
    arrive(kv.at[i, other], r_kv.at[i, other])
    carry = attend(carry, i, other)
    for d in range(1, outer_n):
        from_line(rec[1], d)
    relay_out(1, (1,))
    relay_out(2, (0,))

    def relay_pair(ref, sem):
        arrive(ref, sem)
        launch(ref, ref, sem, partner)

    for e in range(1, inner_n):
        relay_pair(kv.at[turn_i(e), k], r_kv.at[turn_i(e), k])
    for e in range(1, inner_n):
        for ref, sem in state_pieces(turn_i(e), k):
            relay_pair(ref, sem)
    relay_out(2, (1,))
    relay_out(3, (0,))
    from_pairs(rec[1])
    for e in range(1, inner_n):
        there = turn_i(e)
        carry = attend(carry, there, k)
        arrive(kv.at[there, other], r_kv.at[there, other])
        carry = attend(carry, there, other)
    rows_out = carry[0] / carry[1]
    attend_mixed = (
        rows_out * inverse_rms(rows_out, LANES) * mixer_gain_ref[:, lane(hh)]
    ).astype(bf16)

    def send_mix(p):
        for b in range(blocks):
            home = blocks * k + b == o
            launch(
                mix_send.at[p, b],
                mix_recv.at[p, hh],
                r_mix.at[p, hh],
                dev(blocks * k + b, i, x, o // heads),
                jnp.logical_not(home),
            )

            @pl.when(home)
            def _():
                mix_recv[p, hh] = mix_send[p, b]

    for b in range(blocks):
        mix_send[1, b] = attend_mixed[b * rows : (b + 1) * rows]
    send_mix(1)

    from_partner(rec[1])
    qg = project(lambda s: columns(s, (3, 4)), 2 * LANES).astype(f32)
    for e in range(inner_n):
        for k_ in (k, other):
            if e or k_ is other:
                for ref, sem in state_pieces(turn_i(e), k_):
                    if k_ is other:
                        arrive(ref, sem)

    def forward(s, state):
        i_, o_ = lax.rem(s, inner_n), s // inner_n
        return state * jnp.exp(logs[i_, o_, 0, 0:1, :]) + states[i_, o_, 0].astype(f32)

    def backward(j, state):
        s = n - 1 - j
        i_, o_ = lax.rem(s, inner_n), s // inner_n
        return state * jnp.exp(logs[i_, o_, 1, 0:1, :]) + states[i_, o_, 1].astype(f32)

    nothing = jnp.zeros((LANES, LANES), f32)
    for b in range(blocks):
        there = blocks * k + b
        s = there * inner_n + i
        incoming = (
            lax.fori_loop(0, s, forward, nothing).astype(bf16),
            lax.fori_loop(0, n - 1 - s, backward, nothing).astype(bf16),
        )
        at = slice(b * rows, (b + 1) * rows)
        total = jnp.zeros((rows, LANES), f32)
        within = jnp.zeros((rows, rows), f32)
        for d in range(2):
            keys, totals = near[d]
            probe = (qg[at, :LANES] * jnp.exp(totals[b])).astype(bf16)
            within += jnp.where(masks[d], against(probe, keys[b]), 0.0)
            total += against(probe, incoming[d])
        total += jnp.dot(within.astype(bf16), value[b], preferred_element_type=f32)
        gate = qg[at, LANES:]
        scaled = total * inverse_rms(total, LANES) * chain_gain_ref[:, lane(hh)]
        mix_send[0, b] = (scaled * (gate * jax.nn.sigmoid(gate))).astype(bf16)
    send_mix(0)
    relay_out(3, (1,))

    for h in range(heads):
        for p in range(2):
            arrive(mix_recv.at[p, h], r_mix.at[p, h], heads * k + h != o)
    col_n = out_w.shape[4]
    span = inner_n * col_n
    own_rows = 2 * part_rows
    order = (o, o + 1 - 2 * lax.rem(o, 2), turn_o(2), outer_n - 1 - o)
    assert outer_n == len(order)

    def rows_of(p):
        return jnp.concatenate(
            [
                jnp.concatenate(
                    [
                        mix_recv[p, h, pl.ds(pl.multiple_of(x_ * own_rows, own_rows), own_rows), :]
                        for h in range(heads)
                    ],
                    axis=1,
                )
                for x_ in (1 - x, x)
            ],
            axis=0,
        )

    def partial(c):
        for e in range(inner_n):
            product = jnp.dot(
                all_rows[0], out_w[0, e, order[c]], preferred_element_type=f32
            ) + jnp.dot(all_rows[1], out_w[1, e, order[c]], preferred_element_type=f32)
            for side, target in enumerate((part_far, part_near)):
                for q in range(2):
                    first_row = side * own_rows + q * part_rows
                    target[c, q, :, e * col_n : (e + 1) * col_n] = product[
                        first_row : first_row + part_rows
                    ]

    all_rows = [rows_of(p) for p in range(2)]

    def cross(c):
        arrive(got_far.at[c], r_sum.at[0, c])
        send_x[c] = (part_far[c, k] + got_far[c].astype(f32)).astype(bf16)
        launch(send_x.at[c], got_x.at[c], r_sum.at[1, c], beside)

    for c in range(outer_n):
        for j in range(2):
            for e in range(1, inner_n):
                arrive(*out_piece(j, turn_i(e), order[c]))
        partial(c)
        send_far[c] = part_far[c, other].astype(bf16)
        launch(send_far.at[c], got_far.at[c], r_sum.at[0, c], partner)
        send_near[c] = part_near[c, other].astype(bf16)
        launch(send_near.at[c], got_near.at[c], r_sum.at[2, c], partner)
        if c:
            cross(c - 1)
    cross(outer_n - 1)
    for c in range(outer_n):
        arrive(got_near.at[c], r_sum.at[2, c])
        arrive(got_x.at[c], r_sum.at[1, c])
        out_ref[:, lane(order[c], span)] = (
            part_near[c, k] + got_near[c].astype(f32) + got_x[c].astype(f32)
        )
    drain()
    needed.append(used[0])


def on_device(
    tokens,
    input_gain,
    chain_query,
    forward_gate,
    backward_gate,
    chain_value,
    output_gate,
    forget_rate,
    chain_gain,
    query_down,
    latent_down,
    rotary_down,
    query_latent_gain,
    latent_gain,
    query_up,
    latent_up,
    query_head_gain,
    key_head_gain,
    mixer_gain,
    chain_out,
    attend_out,
):
    n, heads_n = lax.axis_size("sp"), lax.axis_size("tp")
    rows, width = tokens.shape
    depth = chain_query.shape[0]
    heads = query_up.shape[1] // ATT_QK
    outer_n = 2 * heads
    inner_n = n // outer_n
    blocks = outer_n // 2
    half = depth // 2
    units = (query_down.shape[1] + latent_down.shape[1]) // LANES
    part = rows // heads_n
    out_cols = n * chain_out.shape[1]

    inverse = rope_theta ** (-np.arange(0, ROPE_DIM, 2) / ROPE_DIM)

    def table(positions):
        angles = np.tile(positions[:, None] * inverse, (1, 2))
        pad = ((0, 0), (0, LANES - ROPE_DIM))
        return [jnp.asarray(np.pad(f(angles), pad), f32) for f in (np.cos, np.sin)]

    in_row = table(np.arange(rows, dtype=np.float64))
    in_block = table(np.arange(n, dtype=np.float64) * rows)

    def halves(w):
        return w.reshape(2, half, w.shape[1])

    operands = (
        tokens.reshape(heads_n, part, width),
        *[
            halves(w)
            for w in (
                chain_value,
                forward_gate,
                backward_gate,
                chain_query,
                output_gate,
                query_down,
                latent_down,
            )
        ],
        rotary_down.T,
        query_up,
        latent_up,
        chain_out,
        attend_out,
        forget_rate,
        chain_gain[None],
        mixer_gain[None],
        input_gain[None],
        query_latent_gain.reshape(-1, LANES),
        latent_gain.reshape(-1, LANES),
        query_head_gain[None],
        key_head_gain[None],
        *in_row,
        *in_block,
    )
    dma = pltpu.SemaphoreType.DMA
    vmem = pl.BlockSpec(memory_space=pltpu.VMEM)
    tall = blocks * rows
    needed = []
    hbm = pl.BlockSpec(memory_space=pltpu.HBM)
    big = operands[:13]

    def build(sends):
      return pl.pallas_call(
        functools.partial(mixer_kernel, n, heads_n, heads, sends, needed),
        out_shape=jax.ShapeDtypeStruct((part, out_cols), f32),
        in_specs=[hbm] * len(big) + [vmem] * (len(operands) - len(big)),
        out_specs=vmem,
        scratch_shapes=[
            pltpu.VMEM((2, outer_n, part, width // 2), bf16),
            pltpu.VMEM((blocks, heads_n, part, width), bf16),
            pltpu.VMEM((n, tall, depth), bf16),
            pltpu.VMEM((inner_n, outer_n, 5, 2, half, LANES), bf16),
            pltpu.VMEM((2, inner_n, outer_n, 2, half, LANES), bf16),
            pltpu.VMEM((n, depth, 2 * LANES), bf16),
            pltpu.VMEM((units, tall, LANES), bf16),
            pltpu.VMEM(forget_rate.shape, f32),
            pltpu.VMEM((1,) + chain_gain.shape, f32),
            pltpu.VMEM((1,) + mixer_gain.shape, f32),
            pltpu.VMEM(query_up.shape, bf16),
            pltpu.VMEM((latent_up.shape[0], 2 * LANES), bf16),
            pltpu.VMEM((inner_n, 2, 2 * blocks + 1, rows, LANES), bf16),
            pltpu.VMEM((inner_n, outer_n, 2, LANES, LANES), bf16),
            pltpu.VMEM((inner_n, outer_n, 2, 8, LANES), f32),
            pltpu.VMEM((2, blocks, rows, LANES), bf16),
            pltpu.VMEM((2, heads, rows, LANES), bf16),
            pltpu.VMEM((2, inner_n, outer_n) + chain_out.shape, bf16),
            pltpu.VMEM((outer_n, 2, part, out_cols // outer_n), f32),
            pltpu.VMEM((outer_n, 2, part, out_cols // outer_n), f32),
            pltpu.VMEM((outer_n, part, out_cols // outer_n), bf16),
            pltpu.VMEM((outer_n, part, out_cols // outer_n), bf16),
            pltpu.VMEM((outer_n, part, out_cols // outer_n), bf16),
            pltpu.VMEM((outer_n, part, out_cols // outer_n), bf16),
            pltpu.VMEM((outer_n, part, out_cols // outer_n), bf16),
            pltpu.VMEM((outer_n, part, out_cols // outer_n), bf16),
            dma((sends,)),
            dma((2, outer_n)),
            dma((2, blocks, heads_n)),
            dma((2, inner_n, outer_n)),
            dma((2, inner_n)),
            dma((2, inner_n, outer_n)),
            dma((2, inner_n)),
            dma((5,)),
            dma((units,)),
            dma((inner_n, 2)),
            dma((inner_n, 2)),
            dma((inner_n, 2)),
            dma((2, heads)),
            dma((2, inner_n, outer_n)),
            dma((3, outer_n)),
        ]
        + [pltpu.VMEM(a.shape, a.dtype) for a in big]
        + [dma((len(big),))],
        compiler_params=pltpu.CompilerParams(
            collective_id=0, has_side_effects=True, vmem_limit_bytes=VMEM_LIMIT
        ),
      )

    jax.eval_shape(build(200 + 30 * n), *operands)
    held = [pltpu.with_memory_space_constraint(a, pltpu.HBM) for a in operands]
    return build(needed[0])(*held)


def solution(mesh):
    placed = (
        P("sp", None),
        P(),
        P("sp", "tp"),
        P("sp", "tp"),
        P("sp", "tp"),
        P("sp", "tp"),
        P("sp", "tp"),
        P(None, "tp"),
        P("tp"),
        P("sp", None),
        P("sp", None),
        P(),
        P(),
        P(),
        P(None, "tp"),
        P(None, "tp"),
        P(),
        P(),
        P("tp"),
        P("tp", "sp"),
        P("tp", "sp"),
    )
    return jax.shard_map(
        on_device, mesh=mesh, in_specs=placed, out_specs=P(("sp", "tp"), None), check_vma=False
    )
```

```python
import functools

import jax
import jax.numpy as jnp
import numpy as np
from jax import lax
from jax.experimental import pallas as pl
from jax.experimental.pallas import tpu as pltpu
from jax.sharding import PartitionSpec as P

LANES = 128
RING = 54
NOPE_DIM = 128
ROPE_DIM = 64
ATT_QK = 192
HALF = ROPE_DIM // 2

norm_eps = 1e-06
rope_theta = 10000.0
MESH = pl.DeviceIdType.MESH
VMEM_LIMIT = 48 * 1024 * 1024
f32 = jnp.float32
bf16 = jnp.bfloat16


def run_if(condition, act):
    if condition is None:
        act()
    else:
        pl.when(condition)(act)


def both(a, b):
    if a is None:
        return b
    if b is None:
        return a
    return jnp.logical_and(a, b)


def against(a, b):
    return lax.dot_general(a, b, (((1,), (1,)), ((), ())), preferred_element_type=f32)


def inverse_rms(values, size):
    return lax.rsqrt(jnp.sum(values * values, axis=-1, keepdims=True) / size + norm_eps)


def spread(count, start, signed):
    row = lax.broadcasted_iota(jnp.int32, (count, 3 * LANES), 0) - start
    col = lax.broadcasted_iota(jnp.int32, (count, 3 * LANES), 1)
    straight = (col < ATT_QK) & (row == col)
    at = col - 2 * LANES
    low = (at >= 0) & (at < HALF) & (row == NOPE_DIM + HALF + at)
    high = (at >= HALF) & (at < ROPE_DIM) & (row == NOPE_DIM + at - HALF)
    return (
        jnp.where(straight, 1.0, 0.0)
        + jnp.where(low, -1.0 if signed else 1.0, 0.0)
        + jnp.where(high, 1.0, 0.0)
    )


def mixer_kernel(n, heads_n, heads, sends, needed, *refs):
    count = 13
    far, near_by = refs[:count], refs[-count:]
    (
        tok_in,
        wv,
        wf,
        wb,
        wq,
        wg,
        q_down,
        l_down,
        rot_down,
        query_up,
        latent_up,
        chain_out,
        attend_out,
    ) = near_by
    (
        rate_in,
        chain_gain_in,
        mixer_gain_in,
        input_gain,
        query_latent_gain,
        latent_gain,
        query_gain,
        key_gain,
        cos_row,
        sin_row,
        cos_block,
        sin_block,
        out_ref,
        stage,
        tok,
        xs,
        w_all,
        l_all,
        rot_all,
        lat,
        rate_ref,
        chain_gain_ref,
        mixer_gain_ref,
        up_q,
        up_l,
        kv,
        states,
        logs,
        mix_send,
        mix_recv,
        out_w,
        part_far,
        part_near,
        send_far,
        send_near,
        got_far,
        got_near,
        send_x,
        got_x,
        ssem,
        r_tok,
        r_deliver,
        r_lat_w,
        r_lat_p,
        r_rec_w,
        r_rec_p,
        r_small,
        r_lat,
        r_kv,
        r_state,
        r_log,
        r_mix,
        r_out,
        r_sum,
    ) = refs[count:-count]
    mats = (wv, wf, wb, wq, wg)
    groups = ((0, 3), (3, 2))
    outer_n = 2 * heads
    inner_n = n // outer_n
    blocks = outer_n // 2
    part_rows, width = tok_in.shape[1:]
    chunk = width // 2
    rows = part_rows * heads_n
    q_units = q_down.shape[2] // LANES

    me = lax.axis_index("sp")
    t = lax.axis_index("tp")
    o, i = me // inner_n, lax.rem(me, inner_n)
    x, k = t // 2, lax.rem(t, 2)
    other = 1 - k
    at_home = (o // heads) == k
    away = jnp.logical_not(at_home)
    hh = lax.rem(o, heads)

    def dev(o_, i_, x_, k_):
        return {"sp": o_ * inner_n + i_, "tp": x_ * 2 + k_}

    def turn_o(d):
        return lax.rem(o + d, outer_n)

    def turn_i(d):
        return lax.rem(i + d, inner_n)

    def lane(index, size=LANES):
        return pl.ds(pl.multiple_of(index * size, LANES), size)

    peers = [dev(turn_o(d), i, x, r) for d in range(1, outer_n) for r in range(2)]
    peers += [dev(o, turn_i(d), x, k) for d in range(1, inner_n)]
    peers += [{"sp": me, "tp": lax.rem(t + d, heads_n)} for d in range(1, heads_n)]
    fetches = [pltpu.make_async_copy(far[j], near_by[j], ssem.at[min(sends, RING) - 1 - j]) for j in range(count)]
    for fetch in fetches:
        fetch.start()
    barrier = pltpu.get_barrier_semaphore()
    for peer in peers:
        pl.semaphore_signal(barrier, inc=1, device_id=peer, device_id_type=MESH)
    pl.semaphore_wait(barrier, len(peers))

    pending, used, shared_slots = [], [0], set()
    ring = min(sends, RING)

    def copy(src, dst, send_sem, recv_sem, device):
        return pltpu.make_async_remote_copy(
            src_ref=src,
            dst_ref=dst,
            send_sem=send_sem,
            recv_sem=recv_sem,
            device_id=device,
            device_id_type=MESH,
        )

    def launch(src, dst, recv_sem, device, condition=None, index=None):
        if index is None:
            if used[0] < ring:
                index = used[0]
                used[0] += 1
            else:
                at = next(a for a, entry in enumerate(pending) if entry[2] not in shared_slots)
                finished, finish_send, index = pending.pop(at)
                run_if(finished, finish_send)

        def make():
            return copy(src, dst, ssem.at[index], recv_sem, device)

        run_if(condition, lambda: make().start())
        pending.append((condition, lambda: make().wait_send(), index))
        return index

    def by_distance(d, act):
        for there, toward in ((o - d, 1), (o + d, -1)):
            valid = (there >= 0) & (there < outer_n)
            act(jnp.clip(there, 0, outer_n - 1), valid, toward)

    def drain():
        for condition, finish_send, _ in pending:
            run_if(condition, finish_send)

    def arrive(dst, recv_sem, condition=None):
        run_if(
            condition,
            lambda: copy(dst, dst, ssem.at[0], recv_sem, dev(o, i, x, other)).wait_recv(),
        )

    partner = dev(o, i, x, other)
    beside = dev(o, i, 1 - x, k)

    right, left = o + 1 < outer_n, o > 0
    halves = [slice(c * chunk, (c + 1) * chunk) for c in range(2)]
    fetches[0].wait()
    for c, at in enumerate(halves):
        for step, condition in ((1, right), (-1, left)):
            launch(
                tok_in.at[t, :, at],
                stage.at[c, o],
                r_tok.at[c, o],
                dev(o + step, i, x, k),
                condition,
            )

    is_q, is_l = x == 0, x != 0
    extra_o, extra_unit = 1 + x, outer_n + x
    extra = o == extra_o
    for fetch in fetches[6:8]:
        fetch.wait()
    for d in range(1, outer_n):
        there, index = turn_o(d), None
        for source, condition in ((q_down, is_q), (l_down, is_l)):
            index = launch(
                source.at[k, :, lane(there)],
                l_all.at[0, i, o, k],
                r_lat_w.at[0, i, o],
                dev(there, i, x, k),
                condition,
                index,
            )
        shared_slots.add(index)
    launch(
        q_down.at[k, :, lane(extra_unit)],
        l_all.at[1, i, o, k],
        r_lat_w.at[1, i, o],
        dev(extra_o, i, x, k),
        jnp.logical_not(extra),
    )
    for fetch in fetches[1:6] + fetches[8:]:
        fetch.wait()

    def send_weights(g):
        first, count = groups[g]
        for m in range(first, first + count):
            for h in range(heads):
                there = heads * k + h
                for r in range(2):
                    launch(
                        mats[m].at[r, :, h * LANES : (h + 1) * LANES],
                        w_all.at[i, o, m, r],
                        r_rec_w.at[g, i, o],
                        dev(there, i, x, r),
                        there != o,
                    )

    def send_home_weights(g):
        first, count = groups[g]
        for m in range(first, first + count):
            launch(
                mats[m].at[other, :, lane(hh)],
                w_all.at[i, o, m, other],
                r_rec_w.at[g, i, o],
                partner,
                at_home,
            )

    def out_piece(j, i_, o_):
        return out_w.at[j, i_, o_], r_out.at[j, i_, o_]

    outs = (chain_out, attend_out)
    send_home_weights(0)
    for j, (source, target) in enumerate(
        (
            (query_up, up_q),
            (latent_up.at[:, lane(hh, 2 * LANES)], up_l),
            (rate_in, rate_ref),
            (chain_gain_in, chain_gain_ref),
            (mixer_gain_in, mixer_gain_ref),
        )
    ):
        launch(source, target, r_small.at[j], partner, at_home)
    send_home_weights(1)

    @pl.when(is_q)
    def _():
        l_all[0, i, o, k] = q_down[k, :, lane(o)]

    @pl.when(is_l)
    def _():
        l_all[0, i, o, k] = l_down[k, :, lane(o)]

    @pl.when(extra)
    def _():
        l_all[1, i, o, k] = q_down[k, :, lane(extra_unit)]

    @pl.when(at_home)
    def _():
        for m in range(len(mats)):
            w_all[i, o, m, k] = mats[m][k, :, lane(hh)]
        up_q[...] = query_up[...]
        up_l[...] = latent_up[:, lane(hh, 2 * LANES)]
        rate_ref[...] = rate_in[...]
        chain_gain_ref[...] = chain_gain_in[...]
        mixer_gain_ref[...] = mixer_gain_in[...]

    def lat_piece(slot, i_, o_):
        return l_all.at[slot, i_, o_, k], r_lat_w.at[slot, i_, o_]

    def lat_block(slot, i_, half):
        return l_all.at[slot, i_, :, half], r_lat_p.at[slot, i_]

    def rec_piece(g, i_, o_):
        first, count = groups[g]
        return w_all.at[i_, o_, first : first + count, k], r_rec_w.at[g, i_, o_]

    def rec_block(g, i_, half):
        first, count = groups[g]
        return w_all.at[i_, :, first : first + count, half], r_rec_p.at[g, i_]

    def own_line(piece, condition=None, own=None):
        ref, sem = piece[0](i, o)
        if own is not None:
            arrive(ref, sem, own)
        for e in range(1, inner_n):
            launch(ref, ref, sem, dev(o, turn_i(e), x, k), condition)

    def from_line(piece, d, condition=None):
        def act(there, valid, toward):
            valid = both(valid, condition)
            ref, sem = piece[0](i, there)
            arrive(ref, sem, valid)
            for e in range(1, inner_n):
                launch(ref, ref, sem, dev(o, turn_i(e), x, k), valid)

        by_distance(d, act)
        if d == outer_n - 1:
            launch(*pair(piece[1], i, k), partner, condition)

    def pair(block, i_, half):
        ref, sem = block(i_, half)
        return ref, ref, sem

    def from_pairs(piece, condition=None):
        for e in range(1, inner_n):
            for d in range(outer_n):
                arrive(*piece[0](turn_i(e), turn_o(d)), condition)
            launch(*pair(piece[1], turn_i(e), k), partner, condition)

    def from_partner(piece, condition=None):
        for e in range(inner_n):
            arrive(*piece[1](turn_i(e), other), condition)

    def kind(piece, block, which):
        return functools.partial(piece, which), functools.partial(block, which)

    lat_a, lat_b = kind(lat_piece, lat_block, 0), kind(lat_piece, lat_block, 1)
    rec = [kind(rec_piece, rec_block, g) for g in range(2)]
    own_line(lat_a)
    own_line(lat_b, extra)

    for b in range(blocks):

        @pl.when(blocks * k + b == o)
        def _():
            tok[b] = tok_in[...]

    sign_pick = spread(ATT_QK, 0, True)[NOPE_DIM:, LANES:].astype(bf16)
    depth = width // n
    rot_all[...] = (
        lax.dot_general(
            rot_down[...], sign_pick, (((0,), (0,)), ((), ())), preferred_element_type=f32
        )
        .astype(bf16)
        .reshape(n, depth, 2 * LANES)
    )

    own_line(rec[0], None, away)
    for j in range(2):
        for e in range(1, inner_n):
            launch(outs[j], *out_piece(j, i, o), dev(o, turn_i(e), x, k))
    own_line(rec[1], None, away)

    def gains(ref):
        wide = jnp.broadcast_to(ref[...], (8, ATT_QK))
        return jnp.dot(
            wide,
            spread(ATT_QK, 0, False),
            precision=lax.Precision.HIGHEST,
            preferred_element_type=f32,
        )[0:1]

    for j, target in enumerate((up_q, up_l, rate_ref, chain_gain_ref, mixer_gain_ref)):
        arrive(target, r_small.at[j], away)
    up_q[...] = jnp.dot(
        up_q[...],
        spread(heads * ATT_QK, hh * ATT_QK, True).astype(bf16),
        preferred_element_type=f32,
    ).astype(bf16)

    for j in range(2):
        out_w[j, i, o] = outs[j][...]

    def send_out(js=(0, 1)):
        for j in js:
            ref, sem = out_piece(j, i, o)
            for step, condition in ((1, right), (-1, left)):
                launch(outs[j], ref, sem, dev(o + step, i, x, k), condition)

    def relay_out(d, js=(0, 1)):
        for j in js:

            def act(there, valid, toward):
                ref, sem = out_piece(j, i, there)
                arrive(ref, sem, valid)
                if d < outer_n - 1:
                    onward = both(valid, right if toward > 0 else left)
                    launch(ref, ref, sem, dev(o + toward, i, x, k), onward)
                for e in range(1, inner_n):
                    launch(
                        ref, ref, sem, dev(o, turn_i(e), x, k), valid
                    )

            by_distance(d, act)


    def relay_tokens(c, there, valid, toward, last):
        ref, sem = stage.at[c, there], r_tok.at[c, there]
        arrive(ref, sem, valid)
        if not last:
            onward = both(valid, right if toward > 0 else left)
            launch(ref, ref, sem, dev(o + toward, i, x, k), onward)
        core, b = there // blocks, lax.rem(there, blocks)
        at = halves[c]
        target, sem = tok.at[b, t, :, at], r_deliver.at[c, b, t]
        launch(ref, target, sem, dev(o, i, 1 - x, core), valid)
        launch(ref, target, sem, partner, both(valid, core != k))

        @pl.when(both(valid, core == k))
        def _():
            tok[b, t, :, at] = stage[c, there]

    for d in range(1, outer_n):
        for c in range(2):
            by_distance(
                d,
                functools.partial(
                    lambda c, there, valid, toward: relay_tokens(
                        c, there, valid, toward, d == outer_n - 1
                    ),
                    c,
                ),
            )
        if d == 1:
            from_line(lat_a, 1)
            from_line(lat_b, 1, extra)
        if d == outer_n - 2:
            send_weights(0)
            for far_d in range(2, outer_n):
                from_line(lat_a, far_d)
                from_line(lat_b, far_d, extra)

    from_pairs(lat_a)
    from_pairs(lat_b, extra)

    for b in range(blocks):
        there = blocks * k + b
        for d in range(1, heads_n):
            q = lax.rem(t + d, heads_n)
            for c, at in enumerate(halves):
                arrive(tok.at[b, q, :, at], r_deliver.at[c, b, q], there != o)
        wide = jnp.concatenate([tok[b, q].astype(f32) for q in range(heads_n)], axis=0)
        scale = inverse_rms(wide, width)
        normed = (wide * scale * input_gain[...]).astype(bf16)
        for s in range(n):
            xs[s, b * rows : (b + 1) * rows, :] = normed[:, s * depth : (s + 1) * depth]

    def project(rhs, columns):
        def body(s, total):
            return total + jnp.dot(xs[s], rhs(s), preferred_element_type=f32)

        return lax.fori_loop(
            0, n, body, jnp.zeros((blocks * rows, columns), f32), unroll=n <= 8
        ).astype(bf16)

    from_partner(lat_a)
    from_partner(lat_b, extra)
    own_unit = x * q_units + o
    first = project(
        lambda s: jnp.concatenate([l_all[0, lax.rem(s, inner_n), s // inner_n].reshape(depth, LANES), rot_all[s]], axis=1),
        3 * LANES,
    )
    lat[own_unit] = first[:, :LANES]
    rotary = first[:, LANES:].astype(f32)

    @pl.when(extra)
    def _():
        lat[extra_unit] = project(lambda s: l_all[1, lax.rem(s, inner_n), s // inner_n].reshape(depth, LANES), LANES)

    def send_unit(unit, condition=None):
        for d in range(1, outer_n):
            launch(lat.at[unit], lat.at[unit], r_lat.at[unit], dev(turn_o(d), i, x, k), condition)
        launch(lat.at[unit], lat.at[unit], r_lat.at[unit], beside, condition)

    send_unit(own_unit)
    send_unit(extra_unit, extra)
    send_out((0,))
    for d in range(1, outer_n):
        from_line(rec[0], d)


    def relay_unit(there, valid, toward):
        unit = x * q_units + there
        arrive(lat.at[unit], r_lat.at[unit], valid)
        launch(lat.at[unit], lat.at[unit], r_lat.at[unit], beside, valid)

    for d in range(1, outer_n):
        by_distance(d, relay_unit)
    arrive(lat.at[extra_unit], r_lat.at[extra_unit], jnp.logical_not(extra))
    launch(
        lat.at[extra_unit],
        lat.at[extra_unit],
        r_lat.at[extra_unit],
        beside,
        jnp.logical_not(extra),
    )
    send_weights(1)
    send_out((1,))
    from_pairs(rec[0])
    relay_out(1, (0,))

    def shared(ref, sem):
        for e in range(1, inner_n):
            launch(ref, ref, sem, dev(o, turn_i(e), x, k))
        launch(ref, ref, sem, partner)

    def columns(s, mats_here):
        return jnp.concatenate([
                w_all[lax.rem(s, inner_n), s // inner_n, m].reshape(depth, LANES)
                for m in mats_here
            ], axis=1)

    from_partner(rec[0])
    vfb = project(lambda s: columns(s, (0, 1, 2)), 3 * LANES)
    value = [vfb[b * rows : (b + 1) * rows, :LANES] for b in range(blocks)]
    row = lax.broadcasted_iota(jnp.int32, (rows, rows), 0)
    col = lax.broadcasted_iota(jnp.int32, (rows, rows), 1)
    masks = (row >= col, row <= col)

    def direction(d):
        rate = rate_ref[d : d + 1, lane(hh)] / (rows * n)
        logit = vfb[:, (1 + d) * LANES : (2 + d) * LANES].astype(f32)
        key = rate * jax.nn.sigmoid(-logit)
        decay = jnp.log1p(-key)
        total = jnp.dot(
            jnp.where(masks[d], 1.0, 0.0),
            jnp.concatenate([decay[b * rows : (b + 1) * rows] for b in range(blocks)], axis=1),
            precision=lax.Precision.HIGHEST,
            preferred_element_type=f32,
        )
        keys, totals = [], []
        last = (rows - 1, 0)[d]
        for b in range(blocks):
            part = total[:, b * LANES : (b + 1) * LANES]
            full = part[last : last + 1, :]
            near = (key[b * rows : (b + 1) * rows] * jnp.exp(-part)).astype(bf16)
            state = lax.dot_general(
                value[b], near, (((0,), (0,)), ((), ())), preferred_element_type=f32
            )
            states[i, blocks * k + b, d] = (state * jnp.exp(full)).astype(bf16)
            logs[i, blocks * k + b, d] = jnp.broadcast_to(full, (8, LANES))
            keys.append(near)
            totals.append(part)
        return keys, totals

    near = [direction(d) for d in range(2)]

    def state_pieces(i_, k_):
        at = pl.ds(k_ * blocks, blocks)
        return (states.at[i_, at], r_state.at[i_, k_]), (logs.at[i_, at], r_log.at[i_, k_])

    for ref, sem in state_pieces(i, k):
        shared(ref, sem)

    for d in range(outer_n):
        unit = (1 - x) * q_units + turn_o(d)
        arrive(lat.at[unit], r_lat.at[unit])
    far_unit = outer_n + 1 - x
    arrive(lat.at[far_unit], r_lat.at[far_unit])

    cosines, sines = [], []
    for b in range(blocks):
        s = (blocks * k + b) * inner_n + i
        cb, sb = cos_block[pl.ds(s, 1), :], sin_block[pl.ds(s, 1), :]
        cosines.append(cb * cos_row[...] - sb * sin_row[...])
        sines.append(sb * cos_row[...] + cb * sin_row[...])
    cosine = jnp.concatenate(cosines, axis=0)
    sine = jnp.concatenate(sines, axis=0)

    def latent(first_unit, count, gain):
        wide = jnp.concatenate(
            [lat[u].astype(f32) for u in range(first_unit, first_unit + count)], axis=1
        )
        scaling = jnp.concatenate([gain[u : u + 1] for u in range(count)], axis=1)
        return (wide * inverse_rms(wide, count * LANES) * scaling).astype(bf16)

    def finish(plain, tail, swapped, gain):
        square = jnp.sum(plain * plain + tail * tail, axis=-1, keepdims=True)
        scale = lax.rsqrt(square / ATT_QK + norm_eps)
        turned = tail * gain[:, LANES : 2 * LANES] * cosine + swapped * gain[:, 2 * LANES :] * sine
        return (plain * scale * gain[:, :LANES]).astype(bf16), turned * scale

    pairs = jnp.dot(
        latent(q_units, outer_n, latent_gain), up_l[...], preferred_element_type=f32
    ).astype(bf16)
    key_plain, key_turned = finish(
        pairs[:, :LANES].astype(f32), rotary[:, :LANES], rotary[:, LANES:], gains(key_gain)
    )
    assert blocks * ROPE_DIM == LANES
    packed = jnp.zeros((rows, LANES), f32)
    for b in range(blocks):
        at = slice(b * rows, (b + 1) * rows)
        kv[i, k, b] = key_plain[at]
        kv[i, k, blocks + b] = pairs[at, LANES:]
        part = key_turned[at]
        packed += pltpu.roll(part, b * ROPE_DIM, axis=1) if b else part
    kv[i, k, 2 * blocks] = packed.astype(bf16)

    shared(kv.at[i, k], r_kv.at[i, k])

    attend_q = (
        jnp.dot(latent(0, q_units, query_latent_gain), up_q[...], preferred_element_type=f32)
        .astype(bf16)
        .astype(f32)
    )
    query_plain, query_turned = finish(
        attend_q[:, :LANES],
        attend_q[:, LANES : 2 * LANES],
        attend_q[:, 2 * LANES :],
        gains(query_gain),
    )
    queries = [
        jnp.concatenate(
            [
                query_plain,
                (pltpu.roll(query_turned, b * ROPE_DIM, axis=1) if b else query_turned).astype(bf16),
            ],
            axis=1,
        )
        for b in range(blocks)
    ]


    scale = ATT_QK ** (-0.5) * 1.4426950408889634

    def attend(carry, i_, k_):
        numer, denom = carry
        for b in range(blocks):
            key = jnp.concatenate([kv[i_, k_, b], kv[i_, k_, 2 * blocks]], axis=1)
            weight = jnp.exp2(against(queries[b], key) * scale)
            numer += jnp.dot(
                weight.astype(bf16), kv[i_, k_, blocks + b], preferred_element_type=f32
            )
            denom += jnp.sum(weight, axis=-1, keepdims=True)
        return numer, denom

    carry = (jnp.zeros((blocks * rows, LANES), f32), jnp.zeros((blocks * rows, 1), f32))
    carry = attend(carry, i, k)
    arrive(kv.at[i, other], r_kv.at[i, other])
    carry = attend(carry, i, other)
    for d in range(1, outer_n):
        from_line(rec[1], d)
    relay_out(1, (1,))
    relay_out(2, (0,))

    def relay_pair(ref, sem):
        arrive(ref, sem)
        launch(ref, ref, sem, partner)

    for e in range(1, inner_n):
        relay_pair(kv.at[turn_i(e), k], r_kv.at[turn_i(e), k])
    for e in range(1, inner_n):
        for ref, sem in state_pieces(turn_i(e), k):
            relay_pair(ref, sem)
    relay_out(2, (1,))
    relay_out(3, (0,))
    from_pairs(rec[1])
    for e in range(1, inner_n):
        there = turn_i(e)
        carry = attend(carry, there, k)
        arrive(kv.at[there, other], r_kv.at[there, other])
        carry = attend(carry, there, other)
    rows_out = carry[0] / carry[1]
    attend_mixed = (
        rows_out * inverse_rms(rows_out, LANES) * mixer_gain_ref[:, lane(hh)]
    ).astype(bf16)

    def send_mix(p):
        for b in range(blocks):
            home = blocks * k + b == o
            launch(
                mix_send.at[p, b],
                mix_recv.at[p, hh],
                r_mix.at[p, hh],
                dev(blocks * k + b, i, x, o // heads),
                jnp.logical_not(home),
            )

            @pl.when(home)
            def _():
                mix_recv[p, hh] = mix_send[p, b]

    for b in range(blocks):
        mix_send[1, b] = attend_mixed[b * rows : (b + 1) * rows]
    send_mix(1)

    from_partner(rec[1])
    qg = project(lambda s: columns(s, (3, 4)), 2 * LANES).astype(f32)
    for e in range(inner_n):
        for k_ in (k, other):
            if e or k_ is other:
                for ref, sem in state_pieces(turn_i(e), k_):
                    if k_ is other:
                        arrive(ref, sem)

    def forward(s, state):
        i_, o_ = lax.rem(s, inner_n), s // inner_n
        return state * jnp.exp(logs[i_, o_, 0, 0:1, :]) + states[i_, o_, 0].astype(f32)

    def backward(j, state):
        s = n - 1 - j
        i_, o_ = lax.rem(s, inner_n), s // inner_n
        return state * jnp.exp(logs[i_, o_, 1, 0:1, :]) + states[i_, o_, 1].astype(f32)

    nothing = jnp.zeros((LANES, LANES), f32)
    for b in range(blocks):
        there = blocks * k + b
        s = there * inner_n + i
        incoming = (
            lax.fori_loop(0, s, forward, nothing).astype(bf16),
            lax.fori_loop(0, n - 1 - s, backward, nothing).astype(bf16),
        )
        at = slice(b * rows, (b + 1) * rows)
        total = jnp.zeros((rows, LANES), f32)
        within = jnp.zeros((rows, rows), f32)
        for d in range(2):
            keys, totals = near[d]
            probe = (qg[at, :LANES] * jnp.exp(totals[b])).astype(bf16)
            within += jnp.where(masks[d], against(probe, keys[b]), 0.0)
            total += against(probe, incoming[d])
        total += jnp.dot(within.astype(bf16), value[b], preferred_element_type=f32)
        gate = qg[at, LANES:]
        scaled = total * inverse_rms(total, LANES) * chain_gain_ref[:, lane(hh)]
        mix_send[0, b] = (scaled * (gate * jax.nn.sigmoid(gate))).astype(bf16)
    send_mix(0)
    relay_out(3, (1,))

    for h in range(heads):
        for p in range(2):
            arrive(mix_recv.at[p, h], r_mix.at[p, h], heads * k + h != o)
    col_n = out_w.shape[4]
    span = inner_n * col_n
    own_rows = 2 * part_rows
    order = (o, o + 1 - 2 * lax.rem(o, 2), turn_o(2), outer_n - 1 - o)
    assert outer_n == len(order)

    def rows_of(p):
        return jnp.concatenate(
            [
                jnp.concatenate(
                    [
                        mix_recv[p, h, pl.ds(pl.multiple_of(x_ * own_rows, own_rows), own_rows), :]
                        for h in range(heads)
                    ],
                    axis=1,
                )
                for x_ in (1 - x, x)
            ],
            axis=0,
        )

    def partial(c):
        for e in range(inner_n):
            product = jnp.dot(
                all_rows[0], out_w[0, e, order[c]], preferred_element_type=f32
            ) + jnp.dot(all_rows[1], out_w[1, e, order[c]], preferred_element_type=f32)
            for side, target in enumerate((part_far, part_near)):
                for q in range(2):
                    first_row = side * own_rows + q * part_rows
                    target[c, q, :, e * col_n : (e + 1) * col_n] = product[
                        first_row : first_row + part_rows
                    ]

    all_rows = [rows_of(p) for p in range(2)]

    def cross(c):
        arrive(got_far.at[c], r_sum.at[0, c])
        send_x[c] = (part_far[c, k] + got_far[c].astype(f32)).astype(bf16)
        launch(send_x.at[c], got_x.at[c], r_sum.at[1, c], beside)

    for c in range(outer_n):
        for j in range(2):
            for e in range(1, inner_n):
                arrive(*out_piece(j, turn_i(e), order[c]))
        partial(c)
        send_far[c] = part_far[c, other].astype(bf16)
        launch(send_far.at[c], got_far.at[c], r_sum.at[0, c], partner)
        send_near[c] = part_near[c, other].astype(bf16)
        launch(send_near.at[c], got_near.at[c], r_sum.at[2, c], partner)
        if c:
            cross(c - 1)
    cross(outer_n - 1)
    for c in range(outer_n):
        arrive(got_near.at[c], r_sum.at[2, c])
        arrive(got_x.at[c], r_sum.at[1, c])
        out_ref[:, lane(order[c], span)] = (
            part_near[c, k] + got_near[c].astype(f32) + got_x[c].astype(f32)
        )
    drain()
    needed.append(used[0])


def on_device(
    tokens,
    input_gain,
    chain_query,
    forward_gate,
    backward_gate,
    chain_value,
    output_gate,
    forget_rate,
    chain_gain,
    query_down,
    latent_down,
    rotary_down,
    query_latent_gain,
    latent_gain,
    query_up,
    latent_up,
    query_head_gain,
    key_head_gain,
    mixer_gain,
    chain_out,
    attend_out,
):
    n, heads_n = lax.axis_size("sp"), lax.axis_size("tp")
    rows, width = tokens.shape
    depth = chain_query.shape[0]
    heads = query_up.shape[1] // ATT_QK
    outer_n = 2 * heads
    inner_n = n // outer_n
    blocks = outer_n // 2
    half = depth // 2
    units = (query_down.shape[1] + latent_down.shape[1]) // LANES
    part = rows // heads_n
    out_cols = n * chain_out.shape[1]

    inverse = rope_theta ** (-np.arange(0, ROPE_DIM, 2) / ROPE_DIM)

    def table(positions):
        angles = np.tile(positions[:, None] * inverse, (1, 2))
        pad = ((0, 0), (0, LANES - ROPE_DIM))
        return [jnp.asarray(np.pad(f(angles), pad), f32) for f in (np.cos, np.sin)]

    in_row = table(np.arange(rows, dtype=np.float64))
    in_block = table(np.arange(n, dtype=np.float64) * rows)

    def halves(w):
        return w.reshape(2, half, w.shape[1])

    operands = (
        tokens.reshape(heads_n, part, width),
        *[
            halves(w)
            for w in (
                chain_value,
                forward_gate,
                backward_gate,
                chain_query,
                output_gate,
                query_down,
                latent_down,
            )
        ],
        rotary_down.T,
        query_up,
        latent_up,
        chain_out,
        attend_out,
        forget_rate,
        chain_gain[None],
        mixer_gain[None],
        input_gain[None],
        query_latent_gain.reshape(-1, LANES),
        latent_gain.reshape(-1, LANES),
        query_head_gain[None],
        key_head_gain[None],
        *in_row,
        *in_block,
    )
    dma = pltpu.SemaphoreType.DMA
    vmem = pl.BlockSpec(memory_space=pltpu.VMEM)
    tall = blocks * rows
    needed = []
    hbm = pl.BlockSpec(memory_space=pltpu.HBM)
    big = operands[:13]

    def build(sends):
      return pl.pallas_call(
        functools.partial(mixer_kernel, n, heads_n, heads, sends, needed),
        out_shape=jax.ShapeDtypeStruct((part, out_cols), f32),
        in_specs=[hbm] * len(big) + [vmem] * (len(operands) - len(big)),
        out_specs=vmem,
        scratch_shapes=[
            pltpu.VMEM((2, outer_n, part, width // 2), bf16),
            pltpu.VMEM((blocks, heads_n, part, width), bf16),
            pltpu.VMEM((n, tall, depth), bf16),
            pltpu.VMEM((inner_n, outer_n, 5, 2, half, LANES), bf16),
            pltpu.VMEM((2, inner_n, outer_n, 2, half, LANES), bf16),
            pltpu.VMEM((n, depth, 2 * LANES), bf16),
            pltpu.VMEM((units, tall, LANES), bf16),
            pltpu.VMEM(forget_rate.shape, f32),
            pltpu.VMEM((1,) + chain_gain.shape, f32),
            pltpu.VMEM((1,) + mixer_gain.shape, f32),
            pltpu.VMEM(query_up.shape, bf16),
            pltpu.VMEM((latent_up.shape[0], 2 * LANES), bf16),
            pltpu.VMEM((inner_n, 2, 2 * blocks + 1, rows, LANES), bf16),
            pltpu.VMEM((inner_n, outer_n, 2, LANES, LANES), bf16),
            pltpu.VMEM((inner_n, outer_n, 2, 8, LANES), f32),
            pltpu.VMEM((2, blocks, rows, LANES), bf16),
            pltpu.VMEM((2, heads, rows, LANES), bf16),
            pltpu.VMEM((2, inner_n, outer_n) + chain_out.shape, bf16),
            pltpu.VMEM((outer_n, 2, part, out_cols // outer_n), f32),
            pltpu.VMEM((outer_n, 2, part, out_cols // outer_n), f32),
            pltpu.VMEM((outer_n, part, out_cols // outer_n), bf16),
            pltpu.VMEM((outer_n, part, out_cols // outer_n), bf16),
            pltpu.VMEM((outer_n, part, out_cols // outer_n), bf16),
            pltpu.VMEM((outer_n, part, out_cols // outer_n), bf16),
            pltpu.VMEM((outer_n, part, out_cols // outer_n), bf16),
            pltpu.VMEM((outer_n, part, out_cols // outer_n), bf16),
            dma((sends,)),
            dma((2, outer_n)),
            dma((2, blocks, heads_n)),
            dma((2, inner_n, outer_n)),
            dma((2, inner_n)),
            dma((2, inner_n, outer_n)),
            dma((2, inner_n)),
            dma((5,)),
            dma((units,)),
            dma((inner_n, 2)),
            dma((inner_n, 2)),
            dma((inner_n, 2)),
            dma((2, heads)),
            dma((2, inner_n, outer_n)),
            dma((3, outer_n)),
        ]
        + [pltpu.VMEM(a.shape, a.dtype) for a in big],
        compiler_params=pltpu.CompilerParams(
            collective_id=0, has_side_effects=True, vmem_limit_bytes=VMEM_LIMIT
        ),
      )

    jax.eval_shape(build(200 + 30 * n), *operands)
    held = [pltpu.with_memory_space_constraint(a, pltpu.HBM) for a in operands]
    return build(needed[0])(*held)


def solution(mesh):
    placed = (
        P("sp", None),
        P(),
        P("sp", "tp"),
        P("sp", "tp"),
        P("sp", "tp"),
        P("sp", "tp"),
        P("sp", "tp"),
        P(None, "tp"),
        P("tp"),
        P("sp", None),
        P("sp", None),
        P(),
        P(),
        P(),
        P(None, "tp"),
        P(None, "tp"),
        P(),
        P(),
        P("tp"),
        P("tp", "sp"),
        P("tp", "sp"),
    )
    return jax.shard_map(
        on_device, mesh=mesh, in_specs=placed, out_specs=P(("sp", "tp"), None), check_vma=False
    )
```
